256 devices in a mesh: ep: 16 (over y, x), tp: 16 (over z, core).
Axes of the slice: x: 4, y: 4, z: 8, core: 2. Of those that a mesh axis runs over, the one named last changes fastest.
Arguments:
- mix_in: bfloat16 [32768, 2048], P(('ep', 'tp')), may hold values from -6 to 6
- mix_gain: float32 [2048], replicated, may hold values from 0.1 to 1.9
- mix_w_in: bfloat16 [2048, 512], P('tp'), may hold values from -0.125 to 0.125
- pool_mat: bfloat16 [4, 128, 128], replicated, may hold values from -0.5 to 0.5
- pool_scale: float32 [512], replicated, may hold values from 0.1 to 1.9
- mix_w_out: bfloat16 [512, 2048], P(None, 'tp'), may hold values from -0.25 to 0.25
- moe_in: bfloat16 [32768, 2048], P(('ep', 'tp')), may hold values from -6 to 6
- moe_gain: float32 [2048], replicated, may hold values from 0.1 to 1.9
- routes: int32 [32768, 2], P('ep'), may hold values from 0 to 255, all different within a row; in each aligned block of 2048 rows (0 to 2047, 2048 to 4095, ...) at most 32 rows name the same one
- route_score: bfloat16 [32768, 2], P('ep'), may hold values from 0.099609375 to 1
- exp_gate: bfloat16 [256, 2048, 768], P(('ep', 'tp')), may hold values from -0.125 to 0.125
- exp_up: bfloat16 [256, 2048, 768], P(('ep', 'tp')), may hold values from -0.125 to 0.125
- exp_down: bfloat16 [256, 768, 2048], P(('ep', 'tp')), may hold values from -0.21875 to 0.21875
- shared_gate: bfloat16 [768, 2048], P('tp'), may hold values from -0.125 to 0.125
- shared_up: bfloat16 [768, 2048], P('tp'), may hold values from -0.125 to 0.125
- shared_down: bfloat16 [768, 2048], P('tp'), may hold values from -0.21875 to 0.21875
Outputs:
- mixed: bfloat16 [32768, 2048], P(('ep', 'tp'))
- moe_out: bfloat16 [32768, 2048], P(('ep', 'tp'))
The draws below stay inside these ranges and needn't reach their ends.
Inputs may be any that keep to these rules, and one draw needn't show every extreme that they name: `routes`: each row names 2 different experts. Within the rows of one index of ep (aligned blocks of 2048 rows) no expert is named more than 32 times, a bound that some expert reaches in some blocks.
All inputs are finite; a program needn't handle non-finite values.
Results may differ from the reference program's by a relative error of at most 0.012.
Values may be sent and summed in bfloat16 or wider, within the bound.
A program may use at most 128 MiB of HBM per device.

```python
import math
import jax
import jax.numpy as jnp
import numpy as np
from jax import lax

D = 2048
GROUP_CH = 128
POOL_GROUPS = 4
POOL = 512
FF = 768
FF_SH = 768
TOP_K = 2
SEQS_MIX = 1
TOK_MOE = 128
EXPERTS = 256
CAP = 32
TOKENS_MIX = 32768
LEN_MIX = 32768
TOKENS_MOE = 32768
N_EP = 16
N_TP = 16


def shard_levels(own_key, shape, shards, low, high):
    def one(axis_at, blocks):
        draws = jax.random.uniform(jax.random.fold_in(jax.random.fold_in(own_key, 6), axis_at), (blocks,), jnp.float32, low / len(shards), high / len(shards))
        return jnp.repeat(jnp.exp(draws), shape[axis_at] // blocks).reshape((-1,) + (1,) * (len(shape) - axis_at - 1))

    level = one(*shards[0])
    for cut in shards[1:]:
        level = level * one(*cut)
    return level


def deal_out(key, own, number, rows, number_of, top, reach, lean):
    sequence = jax.random.permutation(key, number_of)
    crowded, common = portions_of(number_of, rows * top, reach, lean, True), portions_of(number_of, rows * top, reach, lean, False)
    places = jnp.arange(number_of)

    def named(sizes, turn):
        used = int((sizes > 0).sum())
        fixed = max(1, used // 4)
        shifted = fixed + (places - fixed + turn * (used - fixed)) % max(1, number_of - fixed)
        return jnp.zeros((number_of,), jnp.int32).at[sequence[jnp.where(places < fixed, places, shifted)]].set(jnp.asarray(sizes, jnp.int32))

    sizes = jnp.where(number % 4 == 0, named(crowded, number // 4), named(common, number - number // 4 - 1))
    mixed = jax.random.permutation(jax.random.fold_in(own, 3), number_of)
    donor, taker = mixed[0:number_of // 2 * 2:2], mixed[1:number_of // 2 * 2:2]
    margin = jnp.minimum(sizes[donor] - 1, reach - sizes[taker]) // 2
    margin = jnp.where((donor == sequence[0]) | (taker == sequence[0]) | (sizes[taker] == 0), 0, jnp.maximum(margin, 0))
    shifted = jax.random.randint(jax.random.fold_in(own, 4), (number_of // 2,), 0, 1 << 20) % (margin + 1)
    sizes = sizes.at[donor].add(-shifted).at[taker].add(shifted)
    labels = jnp.searchsorted(jnp.cumsum(sizes), jnp.arange(rows * top), side="right").astype(jnp.int32)
    grid = labels.reshape(top, rows).T
    grid = grid[jax.random.permutation(jax.random.fold_in(own, 1), rows)]
    turn = jax.random.randint(jax.random.fold_in(own, 2), (rows, 1), 0, top)
    return jnp.take_along_axis(grid, (jnp.arange(top)[None, :] + turn) % top, axis=1)


def portions_of(amount, total, most, slope, full):
    weights = [(1 << 20) // math.isqrt(rank ** slope) + 1 for rank in range(1, amount + 1)]
    largest = most if full else min(most, max(-(-total // amount), total * weights[0] // sum(weights)))
    least = 1 if total - largest >= amount - 1 else 0
    given, surplus = [largest] + [least] * (amount - 1), total - largest - least * (amount - 1)
    while surplus > 0:
        candidates = [i for i in range(1, amount) if given[i] < largest] or [i for i in range(1, amount) if given[i] < most]
        mass, budget = sum([weights[i] for i in candidates]), surplus
        for i in candidates:
            addition = min(most - given[i], max(1, budget * weights[i] // mass), surplus)
            given[i] = given[i] + addition
            surplus = surplus - addition
    return np.array(given)


def normal_values(rng, shape, spread, most, split=(), kind=jnp.bfloat16):
    array = spread * jax.random.normal(rng, shape, jnp.float32)
    if split:
        array = array * shard_levels(rng, shape, split, -0.22, 0.18)
    return jnp.clip(array, -most, most).astype(kind)


def setup_inputs(seed: int = 0) -> dict:
    arg_keys = jax.random.split(jax.random.key(seed), 17)
    mix_in = normal_values(arg_keys[0], (TOKENS_MIX, D), 1.0, 6.0, ((0, 256),))
    mix_gain = jnp.clip(1.0 + 0.18 * jax.random.normal(arg_keys[1], (D,), jnp.float32), 0.1, 1.9)
    mix_w_in = normal_values(arg_keys[2], (D, POOL), D ** -0.5, 0.125, ((0, 16),))
    pool_mat = normal_values(arg_keys[3], (POOL_GROUPS, GROUP_CH, GROUP_CH), GROUP_CH ** -0.5, 0.5)
    pool_scale = jnp.clip(1.0 + 0.18 * jax.random.normal(arg_keys[4], (POOL,), jnp.float32), 0.1, 1.9)
    mix_w_out = normal_values(arg_keys[5], (POOL, D), POOL ** -0.5, 0.25, ((1, 16),))
    moe_in = normal_values(arg_keys[6], (TOKENS_MOE, D), 1.0, 6.0, ((0, 256),))
    moe_gain = jnp.clip(1.0 + 0.18 * jax.random.normal(arg_keys[7], (D,), jnp.float32), 0.1, 1.9)
    routes_keys = jax.random.split(jax.random.fold_in(arg_keys[8], 1), TOKENS_MOE // (TOK_MOE * N_TP))
    routes_turns = jax.random.permutation(jax.random.fold_in(arg_keys[8], 3), TOKENS_MOE // (TOK_MOE * N_TP))
    routes = jax.vmap(lambda own, number: deal_out(jax.random.fold_in(arg_keys[8], 2), own, number, TOK_MOE * N_TP, EXPERTS, TOP_K, CAP, 2))(routes_keys, routes_turns).reshape((TOKENS_MOE, TOP_K))
    route_score = jnp.clip(jnp.exp(math.log(1.0) - 2.306499 * jax.random.uniform(arg_keys[9], (TOKENS_MOE, TOP_K), jnp.float32) ** shard_levels(arg_keys[9], (TOKENS_MOE, TOP_K), ((0, 16),), -0.2, 0.2)), 0.099609375, 1.0).astype(jnp.bfloat16)
    exp_gate = normal_values(arg_keys[10], (EXPERTS, D, FF), D ** -0.5, 0.125, ((0, 256),))
    exp_up = normal_values(arg_keys[11], (EXPERTS, D, FF), D ** -0.5, 0.125, ((0, 256),))
    exp_down = normal_values(arg_keys[12], (EXPERTS, FF, D), FF ** -0.5, 0.21875, ((0, 256),))
    shared_gate = normal_values(arg_keys[13], (FF_SH, D), D ** -0.5, 0.125, ((0, 16),))
    shared_up = normal_values(arg_keys[14], (FF_SH, D), D ** -0.5, 0.125, ((0, 16),))
    shared_down = normal_values(arg_keys[15], (FF_SH, D), FF_SH ** -0.5, 0.21875, ((0, 16),))
    return dict(mix_in=mix_in, mix_gain=mix_gain, mix_w_in=mix_w_in, pool_mat=pool_mat, pool_scale=pool_scale, mix_w_out=mix_w_out, moe_in=moe_in, moe_gain=moe_gain, routes=routes, route_score=route_score, exp_gate=exp_gate, exp_up=exp_up, exp_down=exp_down, shared_gate=shared_gate, shared_up=shared_up, shared_down=shared_down)


NORM_EPS = 1e-06
ROUTED_SCALE = 2.5

def rms_rows(values, gain):
    floats = values.astype(jnp.float32)
    scaled = floats * lax.rsqrt(lax.optimization_barrier(jnp.mean(floats * floats, axis=-1, keepdims=True)) + NORM_EPS)
    return (scaled * gain.astype(jnp.float32)).astype(jnp.bfloat16)

def expert_ffn(rows_in, w_gate, w_up, w_down):
    gate_act = jnp.dot(rows_in, w_gate, preferred_element_type=jnp.float32)
    up_act = jnp.dot(rows_in, w_up, preferred_element_type=jnp.float32)
    hidden = (jax.nn.silu(gate_act) * up_act).astype(jnp.bfloat16)
    return jnp.dot(hidden, w_down, preferred_element_type=jnp.float32).astype(jnp.bfloat16)

def mixer_ref(mix_in, mix_gain, mix_w_in, pool_mat, pool_scale, mix_w_out):
    normed = rms_rows(mix_in, mix_gain)
    projected = jnp.dot(normed, mix_w_in, preferred_element_type=jnp.float32).astype(jnp.bfloat16)
    channels = projected.shape[1]
    reach_rows = 2 ** POOL_GROUPS - 1
    floats = projected.astype(jnp.float32).reshape(SEQS_MIX, LEN_MIX, channels)
    padded = jnp.pad(floats, ((0, 0), (reach_rows, 0), (0, 0)))
    position = jnp.arange(LEN_MIX, dtype=jnp.int32)
    pieces = []
    for group in range(POOL_GROUPS):
        window_len = 2 ** (group + 1)
        lower = group * GROUP_CH
        upper = lower + GROUP_CH
        running = jnp.zeros((SEQS_MIX, LEN_MIX, GROUP_CH), jnp.float32)
        for offset in range(window_len):
            running = running + padded[:, reach_rows - offset:reach_rows - offset + LEN_MIX, lower:upper]
        counts = jnp.minimum(position + 1, window_len).astype(jnp.float32)
        pieces.append(running / counts[None, :, None] - floats[:, :, lower:upper])
    pooled = jnp.concatenate(pieces, axis=2).astype(jnp.bfloat16).reshape(-1, POOL_GROUPS, GROUP_CH)
    grouped = jnp.einsum('tgc,gcd->tgd', pooled.astype(jnp.float32), pool_mat.astype(jnp.float32))
    pool_out = (grouped.reshape(-1, channels) * pool_scale).astype(jnp.bfloat16)
    return jnp.dot(pool_out, mix_w_out, preferred_element_type=jnp.float32).astype(jnp.bfloat16)

def experts_ref(moe_in, moe_gain, routes, route_score, exp_gate, exp_up, exp_down, shared_gate, shared_up, shared_down):
    normed = rms_rows(moe_in, moe_gain)
    total_rows, model_width = normed.shape
    block_rows = TOK_MOE * N_TP
    per_block = block_rows * TOP_K
    scores = route_score.astype(jnp.float32)
    weights = scores / lax.optimization_barrier(jnp.sum(scores, axis=1, keepdims=True)) * ROUTED_SCALE
    flat_expert = routes.reshape(N_EP, per_block)
    onehot = (flat_expert[:, :, None] == jnp.arange(EXPERTS, dtype=jnp.int32)[None, None, :]).astype(jnp.int32)
    before = lax.optimization_barrier(jnp.sum((jnp.cumsum(onehot, axis=1) - onehot) * onehot, axis=2))
    block_id = jnp.arange(N_EP, dtype=jnp.int32)[:, None]
    slot_span = N_EP * CAP
    flat_slot = (flat_expert * slot_span + block_id * CAP + before).reshape(-1).astype(jnp.int32)
    token_id = (block_id * block_rows + jnp.arange(per_block, dtype=jnp.int32)[None, :] // TOP_K).reshape(-1)
    table = jnp.full((EXPERTS * slot_span,), total_rows, jnp.int32).at[flat_slot].set(token_id)
    table = table.reshape(EXPERTS, slot_span)
    table_weight = jnp.zeros((EXPERTS * slot_span,), jnp.float32).at[flat_slot].set(weights.reshape(-1))
    table_weight = table_weight.reshape(EXPERTS, slot_span)
    padded_rows = jnp.concatenate([normed, jnp.zeros((1, model_width), jnp.bfloat16)], axis=0)
    gate_act = jnp.dot(normed, shared_gate.T, preferred_element_type=jnp.float32)
    up_act = jnp.dot(normed, shared_up.T, preferred_element_type=jnp.float32)
    shared_hidden = (jax.nn.silu(gate_act) * up_act).astype(jnp.bfloat16)
    shared_out = jnp.dot(shared_hidden, shared_down, preferred_element_type=jnp.float32)

    def column_sum(running, column):

        def one_expert(partial_value, ep_rank):
            expert = ep_rank * N_TP + column
            ids = table[expert]
            rows_in = jnp.take(padded_rows, ids, axis=0)
            outputs = expert_ffn(rows_in, exp_gate[expert], exp_up[expert], exp_down[expert])
            partial_value = partial_value.at[ids].add(outputs.astype(jnp.float32) * table_weight[expert][:, None], mode='drop')
            return (partial_value, None)
        partial_value = jnp.zeros((total_rows, model_width), jnp.float32)
        partial_value, _ = lax.scan(one_expert, partial_value, jnp.arange(N_EP, dtype=jnp.int32))
        return (running + partial_value.astype(jnp.bfloat16).astype(jnp.float32), None)
    running, _ = lax.scan(column_sum, jnp.zeros((total_rows, model_width), jnp.float32), jnp.arange(N_TP, dtype=jnp.int32))
    return (running + shared_out).astype(jnp.bfloat16)

def reference(mix_in, mix_gain, mix_w_in, pool_mat, pool_scale, mix_w_out, moe_in, moe_gain, routes, route_score, exp_gate, exp_up, exp_down, shared_gate, shared_up, shared_down):
    mixed = mixer_ref(mix_in, mix_gain, mix_w_in, pool_mat, pool_scale, mix_w_out)
    moe_out = experts_ref(moe_in, moe_gain, routes, route_score, exp_gate, exp_up, exp_down, shared_gate, shared_up, shared_down)
    return (mixed, moe_out)
```

```python
import functools

import jax
import jax.numpy as jnp
from jax import lax
from jax.experimental import pallas as pl
from jax.experimental.pallas import tpu as pltpu
from jax.sharding import PartitionSpec as P

NORM_EPS = 1e-06
ROUTED_SCALE = 2.5
MESH = pl.DeviceIdType.MESH
F32 = jnp.float32
BF16 = jnp.bfloat16
HALO = 16
LANES = 128
MIX_AT = 4

NT = (((1,), (1,)), ((), ()))


def dot(a, b):
    return jnp.dot(a, b, preferred_element_type=F32)


def rms_rows(values, gain):
    floats = values.astype(F32)
    scaled = floats * lax.rsqrt(jnp.mean(floats * floats, axis=-1, keepdims=True) + NORM_EPS)
    return (scaled * gain).astype(BF16)


def kernel(
    n_ep, n_tp, n_chunks, cap,
    moe_in, moe_gain, routes, score, mix_gain, pool_mat, pool_scale,
    mix_in, mix_w_in, mix_w_out, exp_gate, exp_up, exp_down, sh_gate, sh_up, sh_down,
    mixed_ref, moe_ref,
    g_buf, out_buf, in_buf, res_buf, ret_buf, sib_buf, up_buf, dn_buf,
    p_mat, s_mat, spread, hid, hid_acc, gate_acc, up_acc, hidden,
    wg, wu, wd, sgu, sd, mx, wi, wo, pool_buf,
    local_sem, ag_send, ag_up, ag_dn, ag_sib, disp_send, disp_recv, ret_send, ret_recv,
    rs_send, rs_sib, rs_up, rs_dn, w_send, w_recv,
):
    tokens, width = moe_in.shape
    cols = width // n_chunks
    n_z = n_tp // 2
    half = tokens // 2
    slots = n_ep * cap
    ff = wd.shape[0]
    n_sh = sh_gate.shape[0]
    ep = lax.axis_index("ep")
    tp = lax.axis_index("tp")
    z = tp // 2
    k = tp % 2
    lin = ep * n_tp + tp

    def at_z(steps):
        return {"tp": ((z + steps + n_z) % n_z) * 2 + k}

    up, dn, sib = at_z(1), at_z(-1), {"tp": z * 2 + 1 - k}

    def ep_peer(offset):
        return {"ep": (ep + offset) % n_ep}

    after = lax.rem(lin + 1, n_ep * n_tp)
    before = lax.rem(lin + n_ep * n_tp - 1, n_ep * n_tp)

    def by_lin(index):
        return {"ep": index // n_tp, "tp": index % n_tp}

    def send(src, dst, send_sem, recv_sem, device):
        pltpu.make_async_remote_copy(
            src_ref=src, dst_ref=dst, send_sem=send_sem, recv_sem=recv_sem,
            device_id=device, device_id_type=MESH,
        ).start()

    def got(ref, sem):
        pltpu.make_async_remote_copy(
            src_ref=ref, dst_ref=ref, send_sem=sem, recv_sem=sem,
            device_id=sib, device_id_type=MESH,
        ).wait_recv()

    def sent(ref, sem):
        pltpu.make_async_remote_copy(
            src_ref=ref, dst_ref=ref, send_sem=sem, recv_sem=sem,
            device_id=sib, device_id_type=MESH,
        ).wait_send()

    barrier = pltpu.get_barrier_semaphore()

    def hello(device):
        pl.semaphore_signal(barrier, inc=1, device_id=device, device_id_type=MESH)

    for steps in range(1, n_z):
        hello(at_z(steps))
    hello(sib)
    hello(by_lin(after))
    hello(by_lin(before))

    @pl.loop(1, n_ep)
    def _(o):
        hello(ep_peer(o))

    q_rows = pl.ds(pl.multiple_of((ep % 4) * 32, 32), 32)
    q_grp = ep // 4
    e_rows = pl.ds(pl.multiple_of(ep * 32, 32), 32)
    loads = [
        pltpu.make_async_copy(
            mix_w_in.at[q_rows, pl.ds(pl.multiple_of(q_grp * LANES, LANES), LANES)],
            wi.at[q_grp, z, k, q_rows, :], local_sem.at[0]),
        pltpu.make_async_copy(mix_w_out.at[e_rows, :], wo.at[z, k, e_rows, :], local_sem.at[1]),
        pltpu.make_async_copy(sh_gate, sgu.at[pl.ds(0, n_sh), :], local_sem.at[2]),
        pltpu.make_async_copy(sh_up, sgu.at[pl.ds(LANES, n_sh), :], local_sem.at[3]),
        pltpu.make_async_copy(sh_down, sd.at[pl.ds(0, n_sh), :], local_sem.at[4]),
        pltpu.make_async_copy(exp_gate.at[0], wg, local_sem.at[5]),
        pltpu.make_async_copy(exp_up.at[0], wu, local_sem.at[6]),
        pltpu.make_async_copy(exp_down.at[0], wd, local_sem.at[7]),
        pltpu.make_async_copy(mix_in, mx.at[pl.ds(HALO, tokens), :], local_sem.at[8]),
    ]
    for load in loads:
        load.start()

    normed = rms_rows(moe_in[...], moe_gain[...])
    for f in range(n_chunks):
        g_buf[f, tp] = normed[:, f * cols:(f + 1) * cols]

    pl.semaphore_wait(barrier, n_z - 1 + 3 + n_ep - 1)

    send(mix_in.at[pl.ds(tokens - HALO, HALO), :], mx.at[pl.ds(0, HALO), :],
         w_send.at[0], w_recv.at[0], by_lin(after))

    def own_pieces(f):
        own = g_buf.at[f, tp]
        send(own, own, ag_send.at[f, 0], ag_up.at[f, 0], up)
        send(own, own, ag_send.at[f, 1], ag_dn.at[f, 0], dn)
        send(own, own, ag_send.at[f, 2], ag_sib.at[f], sib)

    loads[0].wait()
    loads[1].wait()
    wi_own = wi.at[q_grp, z, k, q_rows, :]
    wo_own = wo.at[z, k, e_rows, :]
    for steps in range(1, n_z):
        send(wi_own, wi_own, w_send.at[1], w_recv.at[1], at_z(steps))
        send(wo_own, wo_own, w_send.at[1], w_recv.at[1], at_z(steps))

    def gather_step(i):
        @pl.when(i < n_chunks)
        def _():
            own_pieces(i)

        for hop in range(1, 4):
            f = i - hop

            @pl.when((f >= 0) & (f < n_chunks))
            def _():
                from_dn = g_buf.at[f, ((z - hop + n_z) % n_z) * 2 + k]
                got(from_dn, ag_up.at[f, hop - 1])
                part = from_dn if hop < 3 else from_dn.at[pl.ds(0, half), :]
                send(part, part, ag_send.at[f, 0], ag_up.at[f, hop], up)
                from_up = g_buf.at[f, ((z + hop) % n_z) * 2 + k]
                got(from_up, ag_dn.at[f, hop - 1])
                part2 = from_up if hop < 3 else from_up.at[pl.ds(half, half), :]
                send(part2, part2, ag_send.at[f, 1], ag_dn.at[f, hop], dn)
                send(from_dn, from_dn, ag_send.at[f, 2], ag_sib.at[f], sib)
                send(from_up, from_up, ag_send.at[f, 2], ag_sib.at[f], sib)

        f4 = i - 4

        @pl.when((f4 >= 0) & (f4 < n_chunks))
        def _():
            far = g_buf.at[f4, ((z + 4) % n_z) * 2 + k]
            got(far.at[pl.ds(0, half), :], ag_up.at[f4, 3])
            got(far.at[pl.ds(half, half), :], ag_dn.at[f4, 3])
            send(far, far, ag_send.at[f4, 2], ag_sib.at[f4], sib)

    own_rows = pl.ds(pl.multiple_of(ep * cap, cap), cap)

    def dispatch(f):
        got(g_buf.at[f, pl.ds(0, n_z)], ag_sib.at[f])
        rows_all = g_buf[f].reshape(n_tp * tokens, cols)
        tile = slots // 2

        @pl.loop(0, 2)
        def _(m):
            rows = pl.ds(pl.multiple_of(m * tile, tile), tile)
            out_buf[f, rows, :] = dot(p_mat[rows, :], rows_all).astype(BF16)

        @pl.loop(1, n_ep)
        def _(o):
            to = lax.rem(ep + o, n_ep)
            send(out_buf.at[f, pl.ds(pl.multiple_of(to * cap, cap), cap), :],
                 in_buf.at[f, own_rows, :], disp_send.at[f], disp_recv.at[f], {"ep": to})

        in_buf[f, own_rows, :] = out_buf[f, own_rows, :]

    def shared_up_part(f):
        at = pl.ds(pl.multiple_of(f * cols, cols), cols)
        w = sgu[:, at]

        @pl.loop(0, n_tp // 4)
        def _(m):
            x = g_buf[f, pl.ds(m * 4, 4)].reshape(4 * tokens, cols)
            rows = pl.ds(pl.multiple_of(m * 4 * tokens, 4 * tokens), 4 * tokens)
            part = lax.dot_general(x, w, NT, preferred_element_type=F32)

            @pl.when(f == 0)
            def _():
                hid_acc[rows, :] = part

            @pl.when(f > 0)
            def _():
                hid_acc[rows, :] += part

    def expert_up_part(f):
        got(in_buf.at[f, pl.ds(0, slots - cap), :], disp_recv.at[f])
        at = pl.ds(pl.multiple_of(f * cols, cols), cols)
        tile = slots // 2
        for w, acc in ((wg, gate_acc), (wu, up_acc)):
            @pl.loop(0, 2)
            def _(m):
                rows = pl.ds(pl.multiple_of(m * tile, tile), tile)
                part = dot(in_buf[f, rows, :], w[at, :])

                @pl.when(f == 0)
                def _():
                    acc[rows, :] = part

                @pl.when(f > 0)
                def _():
                    acc[rows, :] += part

    def route_tables():
        lane = lax.broadcasted_iota(jnp.int32, (LANES, slots), 1)
        row = lax.broadcasted_iota(jnp.int32, (LANES, slots), 0)
        spread[0] = (row == lane // cap).astype(BF16)
        spread[1] = (row - n_ep == lane // cap).astype(BF16)
        wants = (lax.broadcasted_iota(jnp.int32, (tokens, slots), 1) % cap).astype(F32)
        rank_of = lax.broadcasted_iota(jnp.int32, (n_ep, cap, tokens), 1).astype(F32)
        ahead = (lax.broadcasted_iota(jnp.int32, (tokens, tokens), 0)
                 < lax.broadcasted_iota(jnp.int32, (tokens, tokens), 1)).astype(BF16)
        named = lax.broadcasted_iota(jnp.int32, (n_ep, tokens), 0) * n_tp + tp

        def block(b, taken):
            at = pl.ds(pl.multiple_of(b * tokens, tokens), tokens)
            pair = routes[:, at]
            marks = score[:, at].astype(F32)
            total = marks[0:1] + marks[1:2]
            first = pair[0:1] == named
            second = pair[1:2] == named
            mine = first | second
            flags = mine.astype(F32)
            place = dot(flags.astype(BF16), ahead) + taken
            code = jnp.where(mine, place, -1.0)
            weight = jnp.where(first, marks[0:1] / total * ROUTED_SCALE,
                               jnp.where(second, marks[1:2] / total * ROUTED_SCALE, 0.0))
            hot = (code[:, None, :] == rank_of).astype(BF16)
            p_mat[:, at] = hot.reshape(slots, tokens)
            both = jnp.concatenate(
                [code, weight, jnp.zeros((LANES - 2 * n_ep, tokens), F32)], axis=0)
            turned = both.T.astype(BF16)
            ranks = dot(turned, spread[0])
            scale = dot(turned, spread[1])
            spot = (b % 2) * n_z + b // 2
            s_mat[pl.ds(pl.multiple_of(spot * tokens, tokens), tokens), :] = jnp.where(
                ranks == wants, scale, 0.0).astype(BF16)
            return taken + jnp.sum(flags, axis=1, keepdims=True)

        lax.fori_loop(0, n_tp, block, jnp.zeros((n_ep, 1), F32))

    gather_step(0)
    sgu[n_sh:LANES, :] = jnp.zeros((LANES - n_sh, width), BF16)
    sgu[LANES + n_sh:, :] = jnp.zeros((LANES - n_sh, width), BF16)
    sd[n_sh:, :] = jnp.zeros((LANES - n_sh, width), BF16)
    gather_step(1)
    route_tables()
    for load in loads[2:]:
        load.wait()

    wi_set = wi.at[q_grp, :, k, q_rows, :]
    wo_set = wo.at[:, k, e_rows, :]

    @pl.loop(2, n_chunks + 7)
    def _(i):
        gather_step(i)

        @pl.when(i == 2)
        def _():
            got(wo.at[pl.ds(0, n_z - 1), 0, pl.ds(0, 64), :], w_recv.at[1])

            @pl.loop(1, n_ep)
            def _(o):
                send(wi_set, wi_set, w_send.at[2], w_recv.at[2], ep_peer(o))
                send(wo_set, wo_set, w_send.at[3], w_recv.at[3], ep_peer(o))

        f5 = i - 5

        @pl.when((f5 >= 0) & (f5 < n_chunks))
        def _():
            dispatch(f5)
            shared_up_part(f5)

        f6 = i - 7

        @pl.when(f6 >= 0)
        def _():
            expert_up_part(f6)

    @pl.loop(0, 4)
    def _(m):
        tile = slots // 4
        rows = pl.ds(pl.multiple_of(m * tile, tile), tile)
        hidden[rows, :] = (jax.nn.silu(gate_acc[rows, :]) * up_acc[rows, :]).astype(BF16)

    def shared_hidden():
        @pl.loop(0, n_tp)
        def _(b):
            rows = pl.ds(pl.multiple_of(b * tokens, tokens), tokens)
            spot = (b % 2) * n_z + b // 2
            both = hid_acc[rows, :]
            hid[pl.ds(pl.multiple_of(spot * tokens, tokens), tokens), :] = (
                jax.nn.silu(both[:, :LANES]) * both[:, LANES:]).astype(BF16)

    def expert_down(f):
        at = pl.ds(pl.multiple_of(f * cols, cols), cols)
        tile = slots // 2

        @pl.loop(0, 2)
        def _(m):
            rows = pl.ds(pl.multiple_of(m * tile, tile), tile)
            res_buf[f, rows, :] = dot(hidden[rows, :], wd[:, at]).astype(BF16)

        @pl.loop(1, n_ep)
        def _(o):
            to = lax.rem(ep + o, n_ep)
            send(res_buf.at[f, pl.ds(pl.multiple_of(to * cap, cap), cap), :],
                 ret_buf.at[f, own_rows, :], ret_send.at[f], ret_recv.at[f], {"ep": to})

        ret_buf[f, own_rows, :] = res_buf[f, own_rows, :]

    def combine(f):
        got(ret_buf.at[f, pl.ds(0, slots - cap), :], ret_recv.at[f])
        at = pl.ds(pl.multiple_of(f * cols, cols), cols)
        back = ret_buf[f]
        down = sd[:, at]

        @pl.loop(0, n_tp // 2)
        def _(m):
            rows = pl.ds(pl.multiple_of(m * 2 * tokens, 2 * tokens), 2 * tokens)
            part = dot(s_mat[rows, :], back) + dot(hid[rows, :], down)
            g_buf[f, pl.ds(m * 2, 2)] = part.astype(BF16).reshape(2, tokens, cols)

        send(g_buf.at[f, pl.ds((1 - k) * n_z, n_z)], sib_buf.at[f],
             rs_send.at[f, 2], rs_sib.at[f], sib)

    def spot_of(steps):
        return (z + steps + n_z) % n_z

    def plus(f, place, rows, other):
        here = g_buf[f, k * n_z + place, rows, :].astype(F32) + other.astype(F32)
        g_buf[f, k * n_z + place, rows, :] = here.astype(BF16)

    every = pl.ds(0, tokens)
    low = pl.ds(0, half)
    high = pl.ds(half, half)

    def scatter_step(i):
        f = i - 6

        @pl.when((f >= 0) & (f < n_chunks))
        def _():
            got(up_buf.at[f, 3], rs_up.at[f, 3])
            got(dn_buf.at[f, 3], rs_dn.at[f, 3])
            at = pl.ds(pl.multiple_of(f * cols, cols), cols)
            moe_ref[:, at] = (g_buf[f, k * n_z + z].astype(F32) + up_buf[f, 3].astype(F32)
                              + dn_buf[f, 3].astype(F32)).astype(BF16)

        for hop in (3, 2, 1):
            f = i - 2 - hop

            @pl.when((f >= 0) & (f < n_chunks))
            def _():
                rows_up = low if hop == 1 else every
                rows_dn = high if hop == 1 else every
                u, d = spot_of(4 - hop), spot_of(hop - 4)
                got(up_buf.at[f, hop - 1, rows_up, :], rs_up.at[f, hop - 1])
                plus(f, u, rows_up, up_buf[f, hop - 1, rows_up, :])
                send(g_buf.at[f, k * n_z + u], up_buf.at[f, hop],
                     rs_send.at[f, 0], rs_up.at[f, hop], up)
                got(dn_buf.at[f, hop - 1, rows_dn, :], rs_dn.at[f, hop - 1])
                plus(f, d, rows_dn, dn_buf[f, hop - 1, rows_dn, :])
                send(g_buf.at[f, k * n_z + d], dn_buf.at[f, hop],
                     rs_send.at[f, 1], rs_dn.at[f, hop], dn)

        f2 = i - 2

        @pl.when((f2 >= 0) & (f2 < n_chunks))
        def _():
            got(sib_buf.at[f2], rs_sib.at[f2])
            far = spot_of(4)
            plus(f2, far, every, sib_buf[f2, far])
            send(g_buf.at[f2, k * n_z + far, low, :], up_buf.at[f2, 0, low, :],
                 rs_send.at[f2, 0], rs_up.at[f2, 0], up)
            send(g_buf.at[f2, k * n_z + far, high, :], dn_buf.at[f2, 0, high, :],
                 rs_send.at[f2, 1], rs_dn.at[f2, 0], dn)

            @pl.loop(5, n_z + 4)
            def _(s):
                place = lax.rem(z + s, n_z)
                plus(f2, place, every, sib_buf[f2, place])

    def mixer():
        got(wi.at[:, :, 1 - k], w_recv.at[4])
        got(wo.at[:, 1 - k], w_recv.at[5])
        got(mx.at[pl.ds(0, HALO), :], w_recv.at[0])
        rows = rms_rows(mx[...], mix_gain[...])
        position = lin * tokens + lax.broadcasted_iota(jnp.int32, (tokens, LANES), 0)
        inside = (lax.broadcasted_iota(jnp.int32, (tokens + HALO, LANES), 0) >= HALO) | (lin > 0)
        for g in range(4):
            w = wi[g].reshape(width, LANES)
            projected = dot(rows, w).astype(BF16).astype(F32)
            projected = jnp.where(inside, projected, 0.0)
            run = projected
            for step in range(g + 1):
                run = run + pltpu.roll(run, 2 ** step, 0)
            counts = jnp.minimum(position + 1, 2 ** (g + 1)).astype(F32)
            pooled = run[HALO:] / counts - projected[HALO:]
            grouped = dot(pooled.astype(BF16), pool_mat[g])
            pool_buf[:, g * LANES:(g + 1) * LANES] = (
                grouped * pool_scale[:, g * LANES:(g + 1) * LANES]).astype(BF16)

        @pl.loop(0, n_tp)
        def _(t):
            at = pl.ds(pl.multiple_of(t * LANES, LANES), LANES)
            mixed_ref[:, at] = dot(pool_buf[...], wo[t // 2, t % 2]).astype(BF16)

    def return_step(i):
        @pl.when(i < n_chunks)
        def _():
            expert_down(i)

    def combine_step(i):
        f1 = i - 1

        @pl.when((f1 >= 0) & (f1 < n_chunks))
        def _():
            combine(f1)

    return_step(0)
    for f in range(n_chunks):
        sent(g_buf.at[f, pl.ds(0, n_z - 1), pl.ds(0, half), :], ag_send.at[f, 0])
        sent(g_buf.at[f, pl.ds(0, n_z - 1), pl.ds(0, half), :], ag_send.at[f, 1])
        sent(g_buf.at[f, pl.ds(0, n_z)], ag_send.at[f, 2])
    shared_hidden()

    @pl.loop(1, n_chunks + 6)
    def _(i):
        return_step(i)
        scatter_step(i)
        combine_step(i)

        @pl.when(i == 1)
        def _():
            got(wo.at[:, 0, pl.ds(0, 32 * (n_ep - 1)), :], w_recv.at[2])
            got(wo.at[:, 0, pl.ds(0, 32 * (n_ep - 1)), :], w_recv.at[3])
            send(wi.at[:, :, k], wi.at[:, :, k], w_send.at[4], w_recv.at[4], sib)
            send(wo.at[:, k], wo.at[:, k], w_send.at[5], w_recv.at[5], sib)

        @pl.when(i == MIX_AT)
        def _():
            mixer()

    for f in range(n_chunks):
        sent(out_buf.at[f, pl.ds(0, slots - cap), :], disp_send.at[f])
        sent(res_buf.at[f, pl.ds(0, slots - cap), :], ret_send.at[f])
        sent(g_buf.at[f, pl.ds(0, n_z - 1), pl.ds(0, half), :], rs_send.at[f, 0])
        sent(g_buf.at[f, pl.ds(0, n_z - 1), pl.ds(0, half), :], rs_send.at[f, 1])
        sent(sib_buf.at[f], rs_send.at[f, 2])
    sent(mx.at[pl.ds(0, HALO), :], w_send.at[0])
    sent(wo.at[pl.ds(0, n_z - 1), 0, pl.ds(0, 64), :], w_send.at[1])
    sent(wo.at[:, 0, pl.ds(0, 32 * (n_ep - 1)), :], w_send.at[2])
    sent(wo.at[:, 0, pl.ds(0, 32 * (n_ep - 1)), :], w_send.at[3])
    sent(wi.at[:, :, k], w_send.at[4])
    sent(wo.at[:, k], w_send.at[5])


def shards(
    n_ep, n_tp, n_chunks,
    mix_in, mix_gain, mix_w_in, pool_mat, pool_scale, mix_w_out, moe_in, moe_gain,
    routes, route_score, exp_gate, exp_up, exp_down, shared_gate, shared_up, shared_down,
):
    tokens, width = moe_in.shape
    cap = 2 * routes.shape[0] * routes.shape[1] // (n_ep * n_tp)
    slots = n_ep * cap
    ff = exp_gate.shape[2]
    cols = width // n_chunks
    n_z = n_tp // 2
    vmem = pl.BlockSpec(memory_space=pltpu.VMEM)
    hbm = pl.BlockSpec(memory_space=pl.ANY)
    dma = pltpu.SemaphoreType.DMA
    big = (n_chunks, n_tp, tokens, cols)
    return pl.pallas_call(
        functools.partial(kernel, n_ep, n_tp, n_chunks, cap),
        out_shape=(
            jax.ShapeDtypeStruct((tokens, width), BF16),
            jax.ShapeDtypeStruct((tokens, width), BF16),
        ),
        in_specs=[vmem] * 7 + [hbm] * 9,
        out_specs=(vmem, vmem),
        scratch_shapes=[
            pltpu.VMEM(big, BF16),
            pltpu.VMEM((n_chunks, slots, cols), BF16),
            pltpu.VMEM((n_chunks, slots, cols), BF16),
            pltpu.VMEM((n_chunks, slots, cols), BF16),
            pltpu.VMEM((n_chunks, slots, cols), BF16),
            pltpu.VMEM((n_chunks, n_z, tokens, cols), BF16),
            pltpu.VMEM((n_chunks, 4, tokens, cols), BF16),
            pltpu.VMEM((n_chunks, 4, tokens, cols), BF16),
            pltpu.VMEM((slots, n_tp * tokens), BF16),
            pltpu.VMEM((n_tp * tokens, slots), BF16),
            pltpu.VMEM((2, LANES, slots), BF16),
            pltpu.VMEM((n_tp * tokens, LANES), BF16),
            pltpu.VMEM((n_tp * tokens, 2 * LANES), F32),
            pltpu.VMEM((slots, ff), F32),
            pltpu.VMEM((slots, ff), F32),
            pltpu.VMEM((slots, ff), BF16),
            pltpu.VMEM((width, ff), BF16),
            pltpu.VMEM((width, ff), BF16),
            pltpu.VMEM((ff, width), BF16),
            pltpu.VMEM((2 * LANES, width), BF16),
            pltpu.VMEM((LANES, width), BF16),
            pltpu.VMEM((tokens + HALO, width), BF16),
            pltpu.VMEM((4, n_z, 2, tokens, LANES), BF16),
            pltpu.VMEM((n_z, 2, 4 * LANES, LANES), BF16),
            pltpu.VMEM((tokens, 4 * LANES), BF16),
            dma((9,)),
            dma((n_chunks, 3)),
            dma((n_chunks, 4)),
            dma((n_chunks, 4)),
            dma((n_chunks,)),
            dma((n_chunks,)),
            dma((n_chunks,)),
            dma((n_chunks,)),
            dma((n_chunks,)),
            dma((n_chunks, 3)),
            dma((n_chunks,)),
            dma((n_chunks, 4)),
            dma((n_chunks, 4)),
            dma((6,)),
            dma((6,)),
        ],
        compiler_params=pltpu.CompilerParams(
            collective_id=0, has_side_effects=True, vmem_limit_bytes=67043328
        ),
    )(
        moe_in, moe_gain.reshape(1, width), routes.T, route_score.T,
        mix_gain.reshape(1, width), pool_mat, pool_scale.reshape(1, -1),
        mix_in, mix_w_in, mix_w_out, exp_gate, exp_up, exp_down,
        shared_gate, shared_up, shared_down,
    )


def solution(mesh):
    n_ep, n_tp = mesh.shape["ep"], mesh.shape["tp"]
    return jax.shard_map(
        functools.partial(shards, n_ep, n_tp, 8),
        mesh=mesh,
        in_specs=(
            P(("ep", "tp"), None),
            P(),
            P("tp", None),
            P(),
            P(),
            P(None, "tp"),
            P(("ep", "tp"), None),
            P(),
            P("ep", None),
            P("ep", None),
            P(("ep", "tp"), None, None),
            P(("ep", "tp"), None, None),
            P(("ep", "tp"), None, None),
            P("tp", None),
            P("tp", None),
            P("tp", None),
        ),
        out_specs=(P(("ep", "tp"), None), P(("ep", "tp"), None)),
        check_vma=False,
    )
```

```python
import functools

import jax
import jax.numpy as jnp
from jax import lax
from jax.experimental import pallas as pl
from jax.experimental.pallas import tpu as pltpu
from jax.sharding import PartitionSpec as P

NORM_EPS = 1e-06
ROUTED_SCALE = 2.5
MESH = pl.DeviceIdType.MESH
F32 = jnp.float32
BF16 = jnp.bfloat16
HALO = 16
LANES = 128

NT = (((1,), (1,)), ((), ()))


def dot(a, b):
    return jnp.dot(a, b, preferred_element_type=F32)


def rms_rows(values, gain):
    floats = values.astype(F32)
    scaled = floats * lax.rsqrt(jnp.mean(floats * floats, axis=-1, keepdims=True) + NORM_EPS)
    return (scaled * gain).astype(BF16)


def kernel(
    n_ep, n_tp, n_chunks, cap,
    moe_in_hbm, moe_gain_hbm, routes_hbm, score_hbm, mix_gain_hbm, pool_mat_hbm, pool_scale_hbm,
    mix_in, mix_w_in, mix_w_out, exp_gate, exp_up, exp_down, sh_gate, sh_up, sh_down,
    mixed_hbm, moe_hbm,
    moe_in, moe_gain, routes, score, mix_gain, pool_mat, pool_scale, mixed_ref, moe_ref, taken_ref,
    g_buf, out_buf, in_buf, res_buf, ret_buf, sib_buf, up_buf, dn_buf,
    p_mat, s_mat, spread, hid, hid_acc, gate_acc, up_acc, hidden,
    wg, wu, wd, sgu, sgt, sd, mx, wi, wo, pool_buf,
    local_sem, out_sem, ag_send, ag_up, ag_dn, ag_sib, disp_send, disp_recv, ret_send, ret_recv,
    rs_send, rs_sib, rs_up, rs_dn, w_send, w_recv,
):
    tokens, width = moe_in.shape
    cols = width // n_chunks
    n_z = n_tp // 2
    half = tokens // 2
    slots = n_ep * cap
    ff = wd.shape[0]
    n_sh = sh_gate.shape[0]
    ep = lax.axis_index("ep")
    tp = lax.axis_index("tp")
    z = tp // 2
    k = tp % 2
    lin = ep * n_tp + tp

    def at_z(steps):
        return {"tp": ((z + steps + n_z) % n_z) * 2 + k}

    up, dn, sib = at_z(1), at_z(-1), {"tp": z * 2 + 1 - k}

    def ep_peer(offset):
        return {"ep": (ep + offset) % n_ep}

    after = lax.rem(lin + 1, n_ep * n_tp)
    before = lax.rem(lin + n_ep * n_tp - 1, n_ep * n_tp)

    def by_lin(index):
        return {"ep": index // n_tp, "tp": index % n_tp}

    def send(src, dst, send_sem, recv_sem, device):
        pltpu.make_async_remote_copy(
            src_ref=src, dst_ref=dst, send_sem=send_sem, recv_sem=recv_sem,
            device_id=device, device_id_type=MESH,
        ).start()

    def got(ref, sem):
        pltpu.make_async_remote_copy(
            src_ref=ref, dst_ref=ref, send_sem=sem, recv_sem=sem,
            device_id=sib, device_id_type=MESH,
        ).wait_recv()

    def sent(ref, sem):
        pltpu.make_async_remote_copy(
            src_ref=ref, dst_ref=ref, send_sem=sem, recv_sem=sem,
            device_id=sib, device_id_type=MESH,
        ).wait_send()

    barrier = pltpu.get_barrier_semaphore()

    def hello(device):
        pl.semaphore_signal(barrier, inc=1, device_id=device, device_id_type=MESH)

    for steps in range(1, n_z):
        hello(at_z(steps))
    hello(sib)
    hello(by_lin(after))
    hello(by_lin(before))

    @pl.loop(1, n_ep)
    def _(o):
        hello(ep_peer(o))

    q_rows = pl.ds(pl.multiple_of((ep % 4) * 32, 32), 32)
    q_grp = ep // 4
    e_rows = pl.ds(pl.multiple_of(ep * 32, 32), 32)
    early = [
        pltpu.make_async_copy(src, dst, local_sem.at[9 + j])
        for j, (src, dst) in enumerate((
            (moe_in_hbm, moe_in), (moe_gain_hbm, moe_gain), (routes_hbm, routes),
            (score_hbm, score), (mix_gain_hbm, mix_gain), (pool_mat_hbm, pool_mat),
            (pool_scale_hbm, pool_scale)))
    ]
    loads = [
        pltpu.make_async_copy(
            mix_w_in.at[q_rows, pl.ds(pl.multiple_of(q_grp * LANES, LANES), LANES)],
            wi.at[q_grp, z, k, q_rows, :], local_sem.at[0]),
        pltpu.make_async_copy(
            mix_w_out.at[e_rows, :], wo.at[z, k, q_grp, q_rows, :], local_sem.at[1]),
        pltpu.make_async_copy(sh_gate, sgu.at[pl.ds(0, n_sh), :], local_sem.at[2]),
        pltpu.make_async_copy(sh_up, sgu.at[pl.ds(LANES, n_sh), :], local_sem.at[3]),
        pltpu.make_async_copy(sh_down, sd.at[pl.ds(0, n_sh), :], local_sem.at[4]),
        pltpu.make_async_copy(exp_gate.at[0], wg, local_sem.at[5]),
        pltpu.make_async_copy(exp_up.at[0], wu, local_sem.at[6]),
        pltpu.make_async_copy(exp_down.at[0], wd, local_sem.at[7]),
        pltpu.make_async_copy(mix_in, mx.at[pl.ds(HALO, tokens), :], local_sem.at[8]),
    ]
    for load in early + loads:
        load.start()
    for load in early:
        load.wait()

    normed = rms_rows(moe_in[...], moe_gain[...])
    for f in range(n_chunks):
        g_buf[f, tp] = normed[:, f * cols:(f + 1) * cols]

    def own_pieces(f):
        own = g_buf.at[f, tp]
        send(own, own, ag_send.at[f, 0], ag_up.at[f, 0], up)
        send(own, own, ag_send.at[f, 1], ag_dn.at[f, 0], dn)
        send(own, own, ag_send.at[f, 2], ag_sib.at[f], sib)

    wi_own = wi.at[q_grp, z, k, q_rows, :]
    wo_own = wo.at[z, k, q_grp, q_rows, :]
    x_at, y_at = ep % 4, ep // 4

    def weights_along_z():
        send(mix_in.at[pl.ds(tokens - HALO, HALO), :], mx.at[pl.ds(0, HALO), :],
             w_send.at[0], w_recv.at[0], by_lin(after))
        loads[0].wait()
        loads[1].wait()
        for steps in range(1, n_z):
            send(wi_own, wi_own, w_send.at[1], w_recv.at[1], at_z(steps))
            send(wo_own, wo_own, w_send.at[1], w_recv.at[1], at_z(steps))

    def along_x(steps):
        return {"ep": y_at * 4 + (x_at + steps) % 4}

    def along_y(steps):
        return {"ep": ((y_at + steps) % 4) * 4 + x_at}

    wi_set = wi.at[q_grp, :, k, q_rows, :]
    wo_set = wo.at[:, k, q_grp, q_rows, :]
    wi_row = wi.at[q_grp, :, k]
    wo_col = wo.at[:, k, :, q_rows, :]
    three = wo.at[:, 0, 0, pl.ds(0, 96), :]
    three_rows = wo.at[:, 0, pl.ds(0, 3)]

    def weights_first():
        got(wo.at[pl.ds(0, n_z - 1), 0, 0, pl.ds(0, 64), :], w_recv.at[1])
        for steps in range(1, 4):
            send(wi_set, wi_set, w_send.at[2], w_recv.at[2], along_x(steps))
            send(wo_set, wo_set, w_send.at[3], w_recv.at[3], along_y(steps))

    def weights_second():
        got(three, w_recv.at[2])
        got(three, w_recv.at[3])
        for steps in range(1, 4):
            send(wi_row, wi_row, w_send.at[6], w_recv.at[6], along_y(steps))
            send(wo_col, wo_col, w_send.at[7], w_recv.at[7], along_x(steps))

    def weights_sibling():
        got(three_rows, w_recv.at[6])
        got(three_rows, w_recv.at[7])
        send(wi.at[:, :, k], wi.at[:, :, k], w_send.at[4], w_recv.at[4], sib)
        send(wo.at[:, k], wo.at[:, k], w_send.at[5], w_recv.at[5], sib)

    def gather_step(i):
        @pl.when(i < n_chunks)
        def _():
            own_pieces(i)

        for hop in range(1, 4):
            f = i - hop

            @pl.when((f >= 0) & (f < n_chunks))
            def _():
                from_dn = g_buf.at[f, ((z - hop + n_z) % n_z) * 2 + k]
                got(from_dn, ag_up.at[f, hop - 1])
                part = from_dn if hop < 3 else from_dn.at[pl.ds(0, half), :]
                send(part, part, ag_send.at[f, 0], ag_up.at[f, hop], up)
                from_up = g_buf.at[f, ((z + hop) % n_z) * 2 + k]
                got(from_up, ag_dn.at[f, hop - 1])
                part2 = from_up if hop < 3 else from_up.at[pl.ds(half, half), :]
                send(part2, part2, ag_send.at[f, 1], ag_dn.at[f, hop], dn)
                send(from_dn, from_dn, ag_send.at[f, 2], ag_sib.at[f], sib)
                send(from_up, from_up, ag_send.at[f, 2], ag_sib.at[f], sib)

        f4 = i - 4

        @pl.when((f4 >= 0) & (f4 < n_chunks))
        def _():
            far = g_buf.at[f4, ((z + 4) % n_z) * 2 + k]
            got(far.at[pl.ds(0, half), :], ag_up.at[f4, 3])
            got(far.at[pl.ds(half, half), :], ag_dn.at[f4, 3])
            send(far, far, ag_send.at[f4, 2], ag_sib.at[f4], sib)

    own_rows = pl.ds(pl.multiple_of(ep * cap, cap), cap)

    def dispatch(f):
        got(g_buf.at[f, pl.ds(0, n_z)], ag_sib.at[f])
        rows_all = g_buf[f].reshape(n_tp * tokens, cols)
        out_buf[f] = dot(p_mat[...], rows_all).astype(BF16)

        @pl.loop(1, n_ep)
        def _(o):
            to = lax.rem(ep + o, n_ep)
            send(out_buf.at[f, pl.ds(pl.multiple_of(to * cap, cap), cap), :],
                 in_buf.at[f, own_rows, :], disp_send.at[f], disp_recv.at[f], {"ep": to})

        in_buf[f, own_rows, :] = out_buf[f, own_rows, :]

    def shared_up(first):
        base = 0 if first else n_chunks // 2

        @pl.loop(0, n_tp // 4)
        def _(m):
            x = jnp.concatenate(
                [g_buf[base + f, pl.ds(m * 4, 4)].reshape(4 * tokens, cols)
                 for f in range(n_chunks // 2)], axis=1)
            rows = pl.ds(pl.multiple_of(m * 4 * tokens, 4 * tokens), 4 * tokens)
            part = dot(x, sgt[base * cols:(base + n_chunks // 2) * cols, :])
            if first:
                hid_acc[rows, :] = part
            else:
                both = hid_acc[rows, :] + part
                units = (jax.nn.silu(both[:, :LANES]) * both[:, LANES:]).astype(BF16)
                for q in range(4):
                    spot = (q % 2) * n_z + m * 2 + q // 2
                    hid[pl.ds(pl.multiple_of(spot * tokens, tokens), tokens), :] = (
                        units[q * tokens:(q + 1) * tokens])

    def expert_up_part(f):
        got(in_buf.at[f, pl.ds(0, slots - cap), :], disp_recv.at[f])
        at = pl.ds(pl.multiple_of(f * cols, cols), cols)
        for w, acc in ((wg, gate_acc), (wu, up_acc)):
            part = dot(in_buf[f], w[at, :])

            @pl.when(f == 0)
            def _():
                acc[...] = part

            @pl.when(f > 0)
            def _():
                acc[...] += part

    def route_tables(b_from, b_to):
        wants = (lax.broadcasted_iota(jnp.int32, (tokens, slots), 1) % cap).astype(F32)
        rank_of = lax.broadcasted_iota(jnp.int32, (n_ep, cap, tokens), 1).astype(F32)
        ahead = (lax.broadcasted_iota(jnp.int32, (tokens, tokens), 0)
                 < lax.broadcasted_iota(jnp.int32, (tokens, tokens), 1)).astype(BF16)
        named = lax.broadcasted_iota(jnp.int32, (n_ep, tokens), 0) * n_tp + tp

        def block(b, taken):
            at = pl.ds(pl.multiple_of(b * tokens, tokens), tokens)
            pair = routes[:, at]
            marks = score[:, at].astype(F32)
            total = marks[0:1] + marks[1:2]
            first = pair[0:1] == named
            second = pair[1:2] == named
            mine = first | second
            flags = mine.astype(F32)
            place = dot(flags.astype(BF16), ahead) + taken
            code = jnp.where(mine, place, -1.0)
            weight = jnp.where(first, marks[0:1] / total * ROUTED_SCALE,
                               jnp.where(second, marks[1:2] / total * ROUTED_SCALE, 0.0))
            hot = (code[:, None, :] == rank_of).astype(BF16)
            p_mat[:, at] = hot.reshape(slots, tokens)
            both = jnp.concatenate(
                [code, weight, jnp.zeros((LANES - 2 * n_ep, tokens), F32)], axis=0)
            turned = both.T.astype(BF16)
            ranks = dot(turned, spread[0])
            scale = dot(turned, spread[1])
            spot = (b % 2) * n_z + b // 2
            s_mat[pl.ds(pl.multiple_of(spot * tokens, tokens), tokens), :] = jnp.where(
                ranks == wants, scale, 0.0).astype(BF16)
            return taken + jnp.sum(flags, axis=1, keepdims=True)

        taken = lax.fori_loop(b_from, b_to, block, taken_ref[:, :1])
        taken_ref[...] = jnp.broadcast_to(taken, taken_ref.shape)

    pl.semaphore_wait(barrier, n_z - 1 + 3 + n_ep - 1)
    gather_step(0)
    weights_along_z()
    lane = lax.broadcasted_iota(jnp.int32, (LANES, slots), 1)
    row = lax.broadcasted_iota(jnp.int32, (LANES, slots), 0)
    spread[0] = (row == lane // cap).astype(BF16)
    spread[1] = (row - n_ep == lane // cap).astype(BF16)
    taken_ref[...] = jnp.zeros_like(taken_ref)
    sgu[n_sh:LANES, :] = jnp.zeros((LANES - n_sh, width), BF16)
    sgu[LANES + n_sh:, :] = jnp.zeros((LANES - n_sh, width), BF16)
    sd[n_sh:, :] = jnp.zeros((LANES - n_sh, width), BF16)
    for load in loads[2:]:
        load.wait()
    for f in range(n_chunks):
        sgt[f * cols:(f + 1) * cols, :] = sgu[:, f * cols:(f + 1) * cols].T

    @pl.loop(1, n_chunks + 7)
    def _(i):
        gather_step(i)

        @pl.when(i == 2)
        def _():
            weights_first()

        @pl.when(i == 4)
        def _():
            weights_second()

        @pl.when(i < 5)
        def _():
            route_tables((i - 1) * (n_tp // 4), i * (n_tp // 4))

        f5 = i - 5

        @pl.when((f5 >= 0) & (f5 < n_chunks))
        def _():
            dispatch(f5)

        f6 = i - 7

        @pl.when(f6 >= 0)
        def _():
            expert_up_part(f6)

        @pl.when(i == n_chunks // 2 + 4)
        def _():
            shared_up(True)

    @pl.loop(0, 4)
    def _(m):
        tile = slots // 4
        rows = pl.ds(pl.multiple_of(m * tile, tile), tile)
        hidden[rows, :] = (jax.nn.silu(gate_acc[rows, :]) * up_acc[rows, :]).astype(BF16)

    def expert_down(f):
        at = pl.ds(pl.multiple_of(f * cols, cols), cols)
        res_buf[f] = dot(hidden[...], wd[:, at]).astype(BF16)

        @pl.loop(1, n_ep)
        def _(o):
            to = lax.rem(ep + o, n_ep)
            send(res_buf.at[f, pl.ds(pl.multiple_of(to * cap, cap), cap), :],
                 ret_buf.at[f, own_rows, :], ret_send.at[f], ret_recv.at[f], {"ep": to})

        ret_buf[f, own_rows, :] = res_buf[f, own_rows, :]

    def combine(f):
        got(ret_buf.at[f, pl.ds(0, slots - cap), :], ret_recv.at[f])
        at = pl.ds(pl.multiple_of(f * cols, cols), cols)
        back = ret_buf[f]
        down = sd[:, at]

        def half_of(core):
            @pl.loop(0, 2)
            def _(j):
                m = core * 2 + j
                many = n_z // 2 * tokens
                rows = pl.ds(pl.multiple_of(m * many, many), many)
                part = dot(s_mat[rows, :], back) + dot(hid[rows, :], down)
                g_buf[f, pl.ds(m * (n_z // 2), n_z // 2)] = (
                    part.astype(BF16).reshape(n_z // 2, tokens, cols))

        half_of(1 - k)
        send(g_buf.at[f, pl.ds((1 - k) * n_z, n_z)], sib_buf.at[f],
             rs_send.at[f, 2], rs_sib.at[f], sib)
        half_of(k)

    def spot_of(steps):
        return (z + steps + n_z) % n_z

    def plus(f, place, rows, other):
        here = g_buf[f, k * n_z + place, rows, :].astype(F32) + other.astype(F32)
        g_buf[f, k * n_z + place, rows, :] = here.astype(BF16)

    every = pl.ds(0, tokens)
    low = pl.ds(0, half)
    high = pl.ds(half, half)

    def scatter_step(i):
        f = i - 6

        @pl.when((f >= 0) & (f < n_chunks))
        def _():
            got(up_buf.at[f, 3], rs_up.at[f, 3])
            got(dn_buf.at[f, 3], rs_dn.at[f, 3])
            at = pl.ds(pl.multiple_of(f * cols, cols), cols)
            moe_ref[:, at] = (g_buf[f, k * n_z + z].astype(F32) + up_buf[f, 3].astype(F32)
                              + dn_buf[f, 3].astype(F32)).astype(BF16)
            pltpu.make_async_copy(moe_ref.at[:, at], moe_hbm.at[:, at], out_sem.at[0]).start()

        for hop in (3, 2, 1):
            f = i - 2 - hop

            @pl.when((f >= 0) & (f < n_chunks))
            def _():
                rows_up = low if hop == 1 else every
                rows_dn = high if hop == 1 else every
                u, d = spot_of(4 - hop), spot_of(hop - 4)
                got(up_buf.at[f, hop - 1, rows_up, :], rs_up.at[f, hop - 1])
                plus(f, u, rows_up, up_buf[f, hop - 1, rows_up, :])
                send(g_buf.at[f, k * n_z + u], up_buf.at[f, hop],
                     rs_send.at[f, 0], rs_up.at[f, hop], up)
                got(dn_buf.at[f, hop - 1, rows_dn, :], rs_dn.at[f, hop - 1])
                plus(f, d, rows_dn, dn_buf[f, hop - 1, rows_dn, :])
                send(g_buf.at[f, k * n_z + d], dn_buf.at[f, hop],
                     rs_send.at[f, 1], rs_dn.at[f, hop], dn)

        f2 = i - 2

        @pl.when((f2 >= 0) & (f2 < n_chunks))
        def _():
            got(sib_buf.at[f2], rs_sib.at[f2])
            far = spot_of(4)
            plus(f2, far, every, sib_buf[f2, far])
            send(g_buf.at[f2, k * n_z + far, low, :], up_buf.at[f2, 0, low, :],
                 rs_send.at[f2, 0], rs_up.at[f2, 0], up)
            send(g_buf.at[f2, k * n_z + far, high, :], dn_buf.at[f2, 0, high, :],
                 rs_send.at[f2, 1], rs_dn.at[f2, 0], dn)

            @pl.loop(5, n_z + 4)
            def _(s):
                place = lax.rem(z + s, n_z)
                plus(f2, place, every, sib_buf[f2, place])

    def mixer_norm():
        got(wi.at[:, :, 1 - k], w_recv.at[4])
        got(wo.at[:, 1 - k], w_recv.at[5])
        got(mx.at[pl.ds(0, HALO), :], w_recv.at[0])
        mx[...] = rms_rows(mx[...], mix_gain[...])

    def mixer_group(g):
        position = lin * tokens + lax.broadcasted_iota(jnp.int32, (tokens, LANES), 0)
        inside = (lax.broadcasted_iota(jnp.int32, (tokens + HALO, LANES), 0) >= HALO) | (lin > 0)
        projected = dot(mx[...], wi[g].reshape(width, LANES)).astype(BF16).astype(F32)
        projected = jnp.where(inside, projected, 0.0)
        run = projected
        for step in range(g + 1):
            run = run + pltpu.roll(run, 2 ** step, 0)
        counts = jnp.minimum(position + 1, 2 ** (g + 1)).astype(F32)
        pooled = run[HALO:] / counts - projected[HALO:]
        grouped = dot(pooled.astype(BF16), pool_mat[g])
        pool_buf[:, g * LANES:(g + 1) * LANES] = (
            grouped * pool_scale[:, g * LANES:(g + 1) * LANES]).astype(BF16)

    def mixer_out(part):
        @pl.loop(part * (n_tp // 4), (part + 1) * (n_tp // 4))
        def _(t):
            at = pl.ds(pl.multiple_of(t * LANES, LANES), LANES)
            w = wo[t // 2, t % 2].reshape(4 * LANES, LANES)
            mixed_ref[:, at] = dot(pool_buf[...], w).astype(BF16)

        cut = width // 4
        at = pl.ds(pl.multiple_of(part * cut, cut), cut)
        pltpu.make_async_copy(mixed_ref.at[:, at], mixed_hbm.at[:, at], out_sem.at[1]).start()

    expert_down(0)
    for f in range(n_chunks):
        sent(g_buf.at[f, pl.ds(0, n_z - 1), pl.ds(0, half), :], ag_send.at[f, 0])
        sent(g_buf.at[f, pl.ds(0, n_z - 1), pl.ds(0, half), :], ag_send.at[f, 1])
        sent(g_buf.at[f, pl.ds(0, n_z)], ag_send.at[f, 2])
    expert_down(1)
    shared_up(False)
    expert_down(2)
    weights_sibling()

    @pl.loop(1, n_chunks + 6)
    def _(i):
        scatter_step(i)

        @pl.when(i <= n_chunks)
        def _():
            combine(i - 1)

        @pl.when(i + 2 < n_chunks)
        def _():
            expert_down(i + 2)

        pl.when(i == n_chunks - 4)(mixer_norm)
        for g in range(4):
            pl.when(i == n_chunks - 3 + g)(functools.partial(mixer_group, g))

        @pl.when((i > n_chunks) & (i <= n_chunks + 4))
        def _():
            mixer_out(i - n_chunks - 1)

    for f in range(n_chunks):
        sent(out_buf.at[f, pl.ds(0, slots - cap), :], disp_send.at[f])
        sent(res_buf.at[f, pl.ds(0, slots - cap), :], ret_send.at[f])
        sent(g_buf.at[f, pl.ds(0, n_z - 1), pl.ds(0, half), :], rs_send.at[f, 0])
        sent(g_buf.at[f, pl.ds(0, n_z - 1), pl.ds(0, half), :], rs_send.at[f, 1])
        sent(sib_buf.at[f], rs_send.at[f, 2])
    sent(mx.at[pl.ds(0, HALO), :], w_send.at[0])
    sent(wo.at[pl.ds(0, n_z - 1), 0, 0, pl.ds(0, 64), :], w_send.at[1])
    sent(three, w_send.at[2])
    sent(three, w_send.at[3])
    sent(three_rows, w_send.at[6])
    sent(three_rows, w_send.at[7])
    pltpu.make_async_copy(moe_ref, moe_hbm, out_sem.at[0]).wait()
    pltpu.make_async_copy(mixed_ref, mixed_hbm, out_sem.at[1]).wait()
    sent(wi.at[:, :, k], w_send.at[4])
    sent(wo.at[:, k], w_send.at[5])


def shards(
    n_ep, n_tp, n_chunks,
    mix_in, mix_gain, mix_w_in, pool_mat, pool_scale, mix_w_out, moe_in, moe_gain,
    routes, route_score, exp_gate, exp_up, exp_down, shared_gate, shared_up, shared_down,
):
    tokens, width = moe_in.shape
    cap = 2 * routes.shape[0] * routes.shape[1] // (n_ep * n_tp)
    slots = n_ep * cap
    ff = exp_gate.shape[2]
    cols = width // n_chunks
    n_z = n_tp // 2
    hbm = pl.BlockSpec(memory_space=pl.ANY)
    dma = pltpu.SemaphoreType.DMA
    big = (n_chunks, n_tp, tokens, cols)
    return pl.pallas_call(
        functools.partial(kernel, n_ep, n_tp, n_chunks, cap),
        out_shape=(
            jax.ShapeDtypeStruct((tokens, width), BF16),
            jax.ShapeDtypeStruct((tokens, width), BF16),
        ),
        in_specs=[hbm] * 16,
        out_specs=(hbm, hbm),
        scratch_shapes=[
            pltpu.VMEM((tokens, width), BF16),
            pltpu.VMEM((1, width), F32),
            pltpu.VMEM((2, routes.shape[0]), jnp.int32),
            pltpu.VMEM((2, routes.shape[0]), BF16),
            pltpu.VMEM((1, width), F32),
            pltpu.VMEM(pool_mat.shape, BF16),
            pltpu.VMEM((1, pool_scale.shape[0]), F32),
            pltpu.VMEM((tokens, width), BF16),
            pltpu.VMEM((tokens, width), BF16),
            pltpu.VMEM((n_ep, LANES), F32),
            pltpu.VMEM(big, BF16),
            pltpu.VMEM((n_chunks, slots, cols), BF16),
            pltpu.VMEM((n_chunks, slots, cols), BF16),
            pltpu.VMEM((n_chunks, slots, cols), BF16),
            pltpu.VMEM((n_chunks, slots, cols), BF16),
            pltpu.VMEM((n_chunks, n_z, tokens, cols), BF16),
            pltpu.VMEM((n_chunks, 4, tokens, cols), BF16),
            pltpu.VMEM((n_chunks, 4, tokens, cols), BF16),
            pltpu.VMEM((slots, n_tp * tokens), BF16),
            pltpu.VMEM((n_tp * tokens, slots), BF16),
            pltpu.VMEM((2, LANES, slots), BF16),
            pltpu.VMEM((n_tp * tokens, LANES), BF16),
            pltpu.VMEM((n_tp * tokens, 2 * LANES), F32),
            pltpu.VMEM((slots, ff), F32),
            pltpu.VMEM((slots, ff), F32),
            pltpu.VMEM((slots, ff), BF16),
            pltpu.VMEM((width, ff), BF16),
            pltpu.VMEM((width, ff), BF16),
            pltpu.VMEM((ff, width), BF16),
            pltpu.VMEM((2 * LANES, width), BF16),
            pltpu.VMEM((width, 2 * LANES), BF16),
            pltpu.VMEM((LANES, width), BF16),
            pltpu.VMEM((tokens + HALO, width), BF16),
            pltpu.VMEM((4, n_z, 2, tokens, LANES), BF16),
            pltpu.VMEM((n_z, 2, 4, LANES, LANES), BF16),
            pltpu.VMEM((tokens, 4 * LANES), BF16),
            dma((16,)),
            dma((2,)),
            dma((n_chunks, 3)),
            dma((n_chunks, 4)),
            dma((n_chunks, 4)),
            dma((n_chunks,)),
            dma((n_chunks,)),
            dma((n_chunks,)),
            dma((n_chunks,)),
            dma((n_chunks,)),
            dma((n_chunks, 3)),
            dma((n_chunks,)),
            dma((n_chunks, 4)),
            dma((n_chunks, 4)),
            dma((8,)),
            dma((8,)),
        ],
        compiler_params=pltpu.CompilerParams(
            collective_id=0, has_side_effects=True, vmem_limit_bytes=67043328
        ),
    )(
        moe_in, moe_gain.reshape(1, width), routes.T, route_score.T,
        mix_gain.reshape(1, width), pool_mat, pool_scale.reshape(1, -1),
        mix_in, mix_w_in, mix_w_out, exp_gate, exp_up, exp_down,
        shared_gate, shared_up, shared_down,
    )


def solution(mesh):
    n_ep, n_tp = mesh.shape["ep"], mesh.shape["tp"]
    return jax.shard_map(
        functools.partial(shards, n_ep, n_tp, 8),
        mesh=mesh,
        in_specs=(
            P(("ep", "tp"), None),
            P(),
            P("tp", None),
            P(),
            P(),
            P(None, "tp"),
            P(("ep", "tp"), None),
            P(),
            P("ep", None),
            P("ep", None),
            P(("ep", "tp"), None, None),
            P(("ep", "tp"), None, None),
            P(("ep", "tp"), None, None),
            P("tp", None),
            P("tp", None),
            P("tp", None),
        ),
        out_specs=(P(("ep", "tp"), None), P(("ep", "tp"), None)),
        check_vma=False,
    )
```

```python
import functools

import jax
import jax.numpy as jnp
from jax import lax
from jax.experimental import pallas as pl
from jax.experimental.pallas import tpu as pltpu
from jax.sharding import PartitionSpec as P

NORM_EPS = 1e-06
ROUTED_SCALE = 2.5
MESH = pl.DeviceIdType.MESH
F32 = jnp.float32
BF16 = jnp.bfloat16
HALO = 16
LANES = 128

LOOK = 1


def dot(a, b):
    return jnp.dot(a, b, preferred_element_type=F32)


def rms_rows(values, gain):
    floats = values.astype(F32)
    scaled = floats * lax.rsqrt(jnp.mean(floats * floats, axis=-1, keepdims=True) + NORM_EPS)
    return (scaled * gain).astype(BF16)


def kernel(
    n_ep, n_tp, n_chunks, cap,
    moe_in_hbm, moe_gain_hbm, routes_hbm, score_hbm, mix_gain_hbm, pool_mat_hbm, pool_scale_hbm,
    mix_in, mix_w_in, mix_w_out, exp_gate, exp_up, exp_down, sh_gate, sh_up, sh_down,
    mixed_ref, moe_ref,
    moe_in, moe_gain, routes, score, mix_gain, pool_mat, pool_scale, taken_ref,
    g_buf, out_buf, in_buf, res_buf, ret_buf, sib_buf, up_buf, dn_buf,
    p_mat, s_mat, spread, hid, hid_acc, gate_acc, up_acc, hidden,
    wg, wu, wd, sgu, sgt, sd, mx, wi, wo, pool_buf,
    local_sem, ag_send, ag_up, ag_dn, ag_sib, disp_send, disp_recv, ret_send, ret_recv,
    rs_send, rs_sib, rs_up, rs_dn, w_send, w_recv,
):
    tokens, width = moe_in.shape
    cols = width // n_chunks
    n_z = n_tp // 2
    half = tokens // 2
    slots = n_ep * cap
    ff = wd.shape[0]
    n_sh = sh_gate.shape[0]
    ep = lax.axis_index("ep")
    tp = lax.axis_index("tp")
    z = tp // 2
    k = tp % 2
    lin = ep * n_tp + tp

    def at_z(steps):
        return {"tp": ((z + steps + n_z) % n_z) * 2 + k}

    up, dn, sib = at_z(1), at_z(-1), {"tp": z * 2 + 1 - k}

    def ep_peer(offset):
        return {"ep": (ep + offset) % n_ep}

    after = lax.rem(lin + 1, n_ep * n_tp)
    before = lax.rem(lin + n_ep * n_tp - 1, n_ep * n_tp)

    def by_lin(index):
        return {"ep": index // n_tp, "tp": index % n_tp}

    def send(src, dst, send_sem, recv_sem, device):
        pltpu.make_async_remote_copy(
            src_ref=src, dst_ref=dst, send_sem=send_sem, recv_sem=recv_sem,
            device_id=device, device_id_type=MESH,
        ).start()

    def got(ref, sem):
        pltpu.make_async_remote_copy(
            src_ref=ref, dst_ref=ref, send_sem=sem, recv_sem=sem,
            device_id=sib, device_id_type=MESH,
        ).wait_recv()

    def sent(ref, sem):
        pltpu.make_async_remote_copy(
            src_ref=ref, dst_ref=ref, send_sem=sem, recv_sem=sem,
            device_id=sib, device_id_type=MESH,
        ).wait_send()

    barrier = pltpu.get_barrier_semaphore()

    def hello(device):
        pl.semaphore_signal(barrier, inc=1, device_id=device, device_id_type=MESH)

    for steps in range(1, n_z):
        hello(at_z(steps))
    hello(sib)
    hello(by_lin(after))
    hello(by_lin(before))

    @pl.loop(1, n_ep)
    def _(o):
        hello(ep_peer(o))

    q_rows = pl.ds(pl.multiple_of((ep % 4) * 32, 32), 32)
    q_grp = ep // 4
    e_rows = pl.ds(pl.multiple_of(ep * 32, 32), 32)
    early = [
        pltpu.make_async_copy(src, dst, local_sem.at[9 + j])
        for j, (src, dst) in enumerate((
            (moe_in_hbm, moe_in), (moe_gain_hbm, moe_gain), (routes_hbm, routes),
            (score_hbm, score), (mix_gain_hbm, mix_gain), (pool_mat_hbm, pool_mat),
            (pool_scale_hbm, pool_scale)))
    ]
    loads = [
        pltpu.make_async_copy(
            mix_w_in.at[q_rows, pl.ds(pl.multiple_of(q_grp * LANES, LANES), LANES)],
            wi.at[q_grp, z, k, q_rows, :], local_sem.at[0]),
        pltpu.make_async_copy(
            mix_w_out.at[e_rows, :], wo.at[z, k, q_grp, q_rows, :], local_sem.at[1]),
        pltpu.make_async_copy(sh_gate, sgu.at[pl.ds(0, n_sh), :], local_sem.at[2]),
        pltpu.make_async_copy(sh_up, sgu.at[pl.ds(LANES, n_sh), :], local_sem.at[3]),
        pltpu.make_async_copy(sh_down, sd.at[pl.ds(0, n_sh), :], local_sem.at[4]),
        pltpu.make_async_copy(exp_gate.at[0], wg, local_sem.at[5]),
        pltpu.make_async_copy(exp_up.at[0], wu, local_sem.at[6]),
        pltpu.make_async_copy(exp_down.at[0], wd, local_sem.at[7]),
        pltpu.make_async_copy(mix_in, mx.at[pl.ds(HALO, tokens), :], local_sem.at[8]),
    ]
    for load in early + loads:
        load.start()
    for load in early[:2]:
        load.wait()

    normed = rms_rows(moe_in[...], moe_gain[...])
    for f in range(n_chunks):
        g_buf[f, tp] = normed[:, f * cols:(f + 1) * cols]

    def own_pieces(f):
        own = g_buf.at[f, tp]
        send(own, own, ag_send.at[f, 0], ag_up.at[f, 0], up)
        send(own, own, ag_send.at[f, 1], ag_dn.at[f, 0], dn)
        send(own, own, ag_send.at[f, 2], ag_sib.at[f], sib)

    wi_own = wi.at[q_grp, z, k, q_rows, :]
    wo_own = wo.at[z, k, q_grp, q_rows, :]
    x_at, y_at = ep % 4, ep // 4

    def weights_along_z():
        for steps in range(1, n_z):
            send(wi_own, wi_own, w_send.at[1], w_recv.at[1], at_z(steps))
            send(wo_own, wo_own, w_send.at[1], w_recv.at[1], at_z(steps))

    def along_x(steps):
        return {"ep": y_at * 4 + (x_at + steps) % 4}

    def along_y(steps):
        return {"ep": ((y_at + steps) % 4) * 4 + x_at}

    wi_set = wi.at[q_grp, :, k, q_rows, :]
    wo_set = wo.at[:, k, q_grp, q_rows, :]
    wi_row = wi.at[q_grp, :, k]
    wo_col = wo.at[:, k, :, q_rows, :]
    three = wo.at[:, 0, 0, pl.ds(0, 96), :]
    three_rows = wo.at[:, 0, pl.ds(0, 3)]

    def weights_first():
        got(wo.at[pl.ds(0, n_z - 1), 0, 0, pl.ds(0, 64), :], w_recv.at[1])
        for steps in range(1, 4):
            send(wi_set, wi_set, w_send.at[2], w_recv.at[2], along_x(steps))
            send(wo_set, wo_set, w_send.at[3], w_recv.at[3], along_y(steps))

    def weights_second():
        got(three, w_recv.at[2])
        got(three, w_recv.at[3])
        for steps in range(1, 4):
            send(wi_row, wi_row, w_send.at[6], w_recv.at[6], along_y(steps))
            send(wo_col, wo_col, w_send.at[7], w_recv.at[7], along_x(steps))

    def weights_sibling():
        got(three_rows, w_recv.at[6])
        got(three_rows, w_recv.at[7])
        send(wi.at[:, :, k], wi.at[:, :, k], w_send.at[4], w_recv.at[4], sib)
        send(wo.at[:, k], wo.at[:, k], w_send.at[5], w_recv.at[5], sib)

    def gather_step(i):
        @pl.when(i + LOOK < n_chunks)
        def _():
            own_pieces(i + LOOK)

        for hop in range(1, 4):
            f = i - hop

            @pl.when((f >= 0) & (f < n_chunks))
            def _():
                from_dn = g_buf.at[f, ((z - hop + n_z) % n_z) * 2 + k]
                got(from_dn, ag_up.at[f, hop - 1])
                part = from_dn if hop < 3 else from_dn.at[pl.ds(0, half), :]
                send(part, part, ag_send.at[f, 0], ag_up.at[f, hop], up)
                from_up = g_buf.at[f, ((z + hop) % n_z) * 2 + k]
                got(from_up, ag_dn.at[f, hop - 1])
                part2 = from_up if hop < 3 else from_up.at[pl.ds(half, half), :]
                send(part2, part2, ag_send.at[f, 1], ag_dn.at[f, hop], dn)
                send(from_dn, from_dn, ag_send.at[f, 2], ag_sib.at[f], sib)
                send(from_up, from_up, ag_send.at[f, 2], ag_sib.at[f], sib)

        f4 = i - 4

        @pl.when((f4 >= 0) & (f4 < n_chunks))
        def _():
            far = g_buf.at[f4, ((z + 4) % n_z) * 2 + k]
            got(far.at[pl.ds(0, half), :], ag_up.at[f4, 3])
            got(far.at[pl.ds(half, half), :], ag_dn.at[f4, 3])
            send(far, far, ag_send.at[f4, 2], ag_sib.at[f4], sib)

    own_rows = pl.ds(pl.multiple_of(ep * cap, cap), cap)

    others = [(ep + step) % n_ep for step in range(1, n_ep)]

    def dispatch(f):
        got(g_buf.at[f, pl.ds(0, n_z)], ag_sib.at[f])
        rows_all = g_buf[f].reshape(n_tp * tokens, cols)
        out_buf[f] = dot(p_mat[...], rows_all).astype(BF16)

        for to in others:
            send(out_buf.at[f, pl.ds(pl.multiple_of(to * cap, cap), cap), :],
                 in_buf.at[f, own_rows, :], disp_send.at[f], disp_recv.at[f], {"ep": to})

        in_buf[f, own_rows, :] = out_buf[f, own_rows, :]

    def shared_up(first):
        base = 0 if first else n_chunks // 2

        @pl.loop(0, n_tp // 4)
        def _(m):
            x = jnp.concatenate(
                [g_buf[base + f, pl.ds(m * 4, 4)].reshape(4 * tokens, cols)
                 for f in range(n_chunks // 2)], axis=1)
            rows = pl.ds(pl.multiple_of(m * 4 * tokens, 4 * tokens), 4 * tokens)
            part = dot(x, sgt[base * cols:(base + n_chunks // 2) * cols, :])
            if first:
                hid_acc[rows, :] = part
            else:
                both = hid_acc[rows, :] + part
                units = (jax.nn.silu(both[:, :LANES]) * both[:, LANES:]).astype(BF16)
                for q in range(4):
                    spot = (q % 2) * n_z + m * 2 + q // 2
                    hid[pl.ds(pl.multiple_of(spot * tokens, tokens), tokens), :] = (
                        units[q * tokens:(q + 1) * tokens])

    def expert_up_part(f):
        got(in_buf.at[f, pl.ds(0, slots - cap), :], disp_recv.at[f])
        at = pl.ds(pl.multiple_of(f * cols, cols), cols)
        for w, acc in ((wg, gate_acc), (wu, up_acc)):
            part = dot(in_buf[f], w[at, :])

            @pl.when(f == 0)
            def _():
                acc[...] = part

            @pl.when(f > 0)
            def _():
                acc[...] += part

    def route_tables(b_from, b_to):
        wants = (lax.broadcasted_iota(jnp.int32, (tokens, slots), 1) % cap).astype(F32)
        rank_of = lax.broadcasted_iota(jnp.int32, (n_ep, cap, tokens), 1).astype(F32)
        ahead = (lax.broadcasted_iota(jnp.int32, (tokens, tokens), 0)
                 < lax.broadcasted_iota(jnp.int32, (tokens, tokens), 1)).astype(BF16)
        named = lax.broadcasted_iota(jnp.int32, (n_ep, tokens), 0) * n_tp + tp

        def block(b, taken):
            at = pl.ds(pl.multiple_of(b * tokens, tokens), tokens)
            pair = routes[:, at]
            marks = score[:, at].astype(F32)
            total = marks[0:1] + marks[1:2]
            first = pair[0:1] == named
            second = pair[1:2] == named
            mine = first | second
            flags = mine.astype(F32)
            place = dot(flags.astype(BF16), ahead) + taken
            code = jnp.where(mine, place, -1.0)
            weight = jnp.where(first, marks[0:1] / total * ROUTED_SCALE,
                               jnp.where(second, marks[1:2] / total * ROUTED_SCALE, 0.0))
            hot = (code[:, None, :] == rank_of).astype(BF16)
            p_mat[:, at] = hot.reshape(slots, tokens)
            both = jnp.concatenate(
                [code, weight, jnp.zeros((LANES - 2 * n_ep, tokens), F32)], axis=0)
            turned = both.T.astype(BF16)
            ranks = dot(turned, spread[0])
            scale = dot(turned, spread[1])
            spot = (b % 2) * n_z + b // 2
            s_mat[pl.ds(pl.multiple_of(spot * tokens, tokens), tokens), :] = jnp.where(
                ranks == wants, scale, 0.0).astype(BF16)
            return taken + jnp.sum(flags, axis=1, keepdims=True)

        taken = lax.fori_loop(b_from, b_to, block, taken_ref[:, :1])
        taken_ref[...] = jnp.broadcast_to(taken, taken_ref.shape)

    pl.semaphore_wait(barrier, n_z - 1 + 3 + n_ep - 1)
    for f in range(LOOK):
        own_pieces(f)
    gather_step(0)
    loads[0].wait()
    loads[1].wait()
    send(mix_in.at[pl.ds(tokens - HALO, HALO), :], mx.at[pl.ds(0, HALO), :],
         w_send.at[0], w_recv.at[0], by_lin(after))
    lane = lax.broadcasted_iota(jnp.int32, (LANES, slots), 1)
    row = lax.broadcasted_iota(jnp.int32, (LANES, slots), 0)
    spread[0] = (row == lane // cap).astype(BF16)
    spread[1] = (row - n_ep == lane // cap).astype(BF16)
    taken_ref[...] = jnp.zeros_like(taken_ref)
    sgu[n_sh:LANES, :] = jnp.zeros((LANES - n_sh, width), BF16)
    sgu[LANES + n_sh:, :] = jnp.zeros((LANES - n_sh, width), BF16)
    sd[n_sh:, :] = jnp.zeros((LANES - n_sh, width), BF16)
    for load in early[2:] + loads[2:]:
        load.wait()
    for f in range(n_chunks):
        sgt[f * cols:(f + 1) * cols, :] = sgu[:, f * cols:(f + 1) * cols].T

    @pl.loop(1, n_chunks + 7)
    def _(i):
        gather_step(i)
        pl.when(i == n_chunks + 2)(weights_along_z)
        pl.when(i == n_chunks + 5)(weights_first)

        @pl.when(i < 5)
        def _():
            route_tables((i - 1) * (n_tp // 4), i * (n_tp // 4))

        f5 = i - 5

        @pl.when((f5 >= 0) & (f5 < n_chunks))
        def _():
            dispatch(f5)

        @pl.when(i == n_chunks + 4)
        def _():
            shared_up(True)

        f6 = i - 7

        @pl.when(f6 >= 0)
        def _():
            expert_up_part(f6)

    @pl.loop(0, 4)
    def _(m):
        tile = slots // 4
        rows = pl.ds(pl.multiple_of(m * tile, tile), tile)
        hidden[rows, :] = (jax.nn.silu(gate_acc[rows, :]) * up_acc[rows, :]).astype(BF16)

    def expert_down(f):
        at = pl.ds(pl.multiple_of(f * cols, cols), cols)
        res_buf[f] = dot(hidden[...], wd[:, at]).astype(BF16)

        for to in others:
            send(res_buf.at[f, pl.ds(pl.multiple_of(to * cap, cap), cap), :],
                 ret_buf.at[f, own_rows, :], ret_send.at[f], ret_recv.at[f], {"ep": to})

        ret_buf[f, own_rows, :] = res_buf[f, own_rows, :]

    def combine(f):
        got(ret_buf.at[f, pl.ds(0, slots - cap), :], ret_recv.at[f])
        at = pl.ds(pl.multiple_of(f * cols, cols), cols)
        back = ret_buf[f]
        down = sd[:, at]

        def half_of(core):
            @pl.loop(0, 2)
            def _(j):
                m = core * 2 + j
                many = n_z // 2 * tokens
                rows = pl.ds(pl.multiple_of(m * many, many), many)
                part = dot(s_mat[rows, :], back) + dot(hid[rows, :], down)
                g_buf[f, pl.ds(m * (n_z // 2), n_z // 2)] = (
                    part.astype(BF16).reshape(n_z // 2, tokens, cols))

        half_of(1 - k)
        send(g_buf.at[f, pl.ds((1 - k) * n_z, n_z)], sib_buf.at[f],
             rs_send.at[f, 2], rs_sib.at[f], sib)
        half_of(k)

    def spot_of(steps):
        return (z + steps + n_z) % n_z

    def plus(f, place, rows, other):
        here = g_buf[f, k * n_z + place, rows, :].astype(F32) + other.astype(F32)
        g_buf[f, k * n_z + place, rows, :] = here.astype(BF16)

    every = pl.ds(0, tokens)
    low = pl.ds(0, half)
    high = pl.ds(half, half)

    def scatter_step(i):
        f = i - 6

        @pl.when((f >= 0) & (f < n_chunks))
        def _():
            got(up_buf.at[f, 3], rs_up.at[f, 3])
            got(dn_buf.at[f, 3], rs_dn.at[f, 3])
            at = pl.ds(pl.multiple_of(f * cols, cols), cols)
            moe_ref[:, at] = (g_buf[f, k * n_z + z].astype(F32) + up_buf[f, 3].astype(F32)
                              + dn_buf[f, 3].astype(F32)).astype(BF16)

        for hop in (3, 2, 1):
            f = i - 2 - hop

            @pl.when((f >= 0) & (f < n_chunks))
            def _():
                rows_up = low if hop == 1 else every
                rows_dn = high if hop == 1 else every
                u, d = spot_of(4 - hop), spot_of(hop - 4)
                got(up_buf.at[f, hop - 1, rows_up, :], rs_up.at[f, hop - 1])
                plus(f, u, rows_up, up_buf[f, hop - 1, rows_up, :])
                send(g_buf.at[f, k * n_z + u], up_buf.at[f, hop],
                     rs_send.at[f, 0], rs_up.at[f, hop], up)
                got(dn_buf.at[f, hop - 1, rows_dn, :], rs_dn.at[f, hop - 1])
                plus(f, d, rows_dn, dn_buf[f, hop - 1, rows_dn, :])
                send(g_buf.at[f, k * n_z + d], dn_buf.at[f, hop],
                     rs_send.at[f, 1], rs_dn.at[f, hop], dn)

        f2 = i - 2

        @pl.when((f2 >= 0) & (f2 < n_chunks))
        def _():
            got(sib_buf.at[f2], rs_sib.at[f2])
            far = spot_of(4)
            plus(f2, far, every, sib_buf[f2, far])
            send(g_buf.at[f2, k * n_z + far, low, :], up_buf.at[f2, 0, low, :],
                 rs_send.at[f2, 0], rs_up.at[f2, 0], up)
            send(g_buf.at[f2, k * n_z + far, high, :], dn_buf.at[f2, 0, high, :],
                 rs_send.at[f2, 1], rs_dn.at[f2, 0], dn)

            @pl.loop(5, n_z + 4)
            def _(s):
                place = lax.rem(z + s, n_z)
                plus(f2, place, every, sib_buf[f2, place])

    def mixer_norm():
        got(wi.at[:, :, 1 - k], w_recv.at[4])
        got(wo.at[:, 1 - k], w_recv.at[5])
        got(mx.at[pl.ds(0, HALO), :], w_recv.at[0])
        mx[...] = rms_rows(mx[...], mix_gain[...])

    def mixer_group(g):
        position = lin * tokens + lax.broadcasted_iota(jnp.int32, (tokens, LANES), 0)
        inside = (lax.broadcasted_iota(jnp.int32, (tokens + HALO, LANES), 0) >= HALO) | (lin > 0)
        projected = dot(mx[...], wi[g].reshape(width, LANES)).astype(BF16).astype(F32)
        projected = jnp.where(inside, projected, 0.0)
        run = projected
        for step in range(g + 1):
            run = run + pltpu.roll(run, 2 ** step, 0)
        counts = jnp.minimum(position + 1, 2 ** (g + 1)).astype(F32)
        pooled = run[HALO:] / counts - projected[HALO:]
        grouped = dot(pooled.astype(BF16), pool_mat[g])
        pool_buf[:, g * LANES:(g + 1) * LANES] = (
            grouped * pool_scale[:, g * LANES:(g + 1) * LANES]).astype(BF16)

    def mixer_out(part):
        @pl.loop(part * (n_tp // 4), (part + 1) * (n_tp // 4))
        def _(t):
            at = pl.ds(pl.multiple_of(t * LANES, LANES), LANES)
            w = wo[t // 2, t % 2].reshape(4 * LANES, LANES)
            mixed_ref[:, at] = dot(pool_buf[...], w).astype(BF16)

    def settle(f):
        sent(res_buf.at[f, pl.ds(0, slots - cap), :], ret_send.at[f])
        sent(g_buf.at[f, pl.ds(0, n_z - 1), pl.ds(0, half), :], rs_send.at[f, 0])
        sent(g_buf.at[f, pl.ds(0, n_z - 1), pl.ds(0, half), :], rs_send.at[f, 1])
        sent(sib_buf.at[f], rs_send.at[f, 2])

    expert_down(0)
    for f in range(n_chunks):
        sent(g_buf.at[f, pl.ds(0, n_z - 1), pl.ds(0, half), :], ag_send.at[f, 0])
        sent(g_buf.at[f, pl.ds(0, n_z - 1), pl.ds(0, half), :], ag_send.at[f, 1])
        sent(g_buf.at[f, pl.ds(0, n_z)], ag_send.at[f, 2])
    expert_down(1)
    shared_up(False)

    @pl.loop(2, 5)
    def _(f):
        expert_down(f)

    @pl.loop(1, n_chunks + 6)
    def _(i):
        scatter_step(i)

        @pl.when(i <= n_chunks)
        def _():
            combine(i - 1)
            sent(out_buf.at[i - 1, pl.ds(0, slots - cap), :], disp_send.at[i - 1])

        @pl.when(i + 4 < n_chunks)
        def _():
            expert_down(i + 4)

        pl.when(i == 3)(weights_second)
        pl.when(i == n_chunks)(weights_sibling)

        @pl.when(i == n_chunks + 1)
        def _():
            mixer_norm()
            mixer_group(0)
            mixer_group(1)

        @pl.when(i == n_chunks + 2)
        def _():
            mixer_group(2)
            mixer_group(3)
            mixer_out(0)

        @pl.when(i == n_chunks + 3)
        def _():
            mixer_out(1)
            mixer_out(2)

        @pl.when(i == n_chunks + 4)
        def _():
            mixer_out(3)

        @pl.when(i > 6)
        def _():
            settle(i - 7)

        @pl.when(i == n_chunks + 4)
        def _():
            sent(mx.at[pl.ds(0, HALO), :], w_send.at[0])
            sent(wo.at[pl.ds(0, n_z - 1), 0, 0, pl.ds(0, 64), :], w_send.at[1])
            sent(three, w_send.at[2])
            sent(three, w_send.at[3])
            sent(three_rows, w_send.at[6])
            sent(three_rows, w_send.at[7])
            sent(wi.at[:, :, k], w_send.at[4])
            sent(wo.at[:, k], w_send.at[5])

    settle(n_chunks - 1)


def shards(
    n_ep, n_tp, n_chunks,
    mix_in, mix_gain, mix_w_in, pool_mat, pool_scale, mix_w_out, moe_in, moe_gain,
    routes, route_score, exp_gate, exp_up, exp_down, shared_gate, shared_up, shared_down,
):
    tokens, width = moe_in.shape
    cap = 2 * routes.shape[0] * routes.shape[1] // (n_ep * n_tp)
    slots = n_ep * cap
    ff = exp_gate.shape[2]
    cols = width // n_chunks
    n_z = n_tp // 2
    hbm = pl.BlockSpec(memory_space=pl.ANY)
    dma = pltpu.SemaphoreType.DMA
    big = (n_chunks, n_tp, tokens, cols)
    return pl.pallas_call(
        functools.partial(kernel, n_ep, n_tp, n_chunks, cap),
        out_shape=(
            pltpu.VMEM((tokens, width), BF16),
            pltpu.VMEM((tokens, width), BF16),
        ),
        in_specs=[hbm] * 16,
        out_specs=(pl.BlockSpec(memory_space=pltpu.VMEM),) * 2,
        scratch_shapes=[
            pltpu.VMEM((tokens, width), BF16),
            pltpu.VMEM((1, width), F32),
            pltpu.VMEM((2, routes.shape[0]), jnp.int32),
            pltpu.VMEM((2, routes.shape[0]), BF16),
            pltpu.VMEM((1, width), F32),
            pltpu.VMEM(pool_mat.shape, BF16),
            pltpu.VMEM((1, pool_scale.shape[0]), F32),
            pltpu.VMEM((n_ep, LANES), F32),
            pltpu.VMEM(big, BF16),
            pltpu.VMEM((n_chunks, slots, cols), BF16),
            pltpu.VMEM((n_chunks, slots, cols), BF16),
            pltpu.VMEM((n_chunks, slots, cols), BF16),
            pltpu.VMEM((n_chunks, slots, cols), BF16),
            pltpu.VMEM((n_chunks, n_z, tokens, cols), BF16),
            pltpu.VMEM((n_chunks, 4, tokens, cols), BF16),
            pltpu.VMEM((n_chunks, 4, tokens, cols), BF16),
            pltpu.VMEM((slots, n_tp * tokens), BF16),
            pltpu.VMEM((n_tp * tokens, slots), BF16),
            pltpu.VMEM((2, LANES, slots), BF16),
            pltpu.VMEM((n_tp * tokens, LANES), BF16),
            pltpu.VMEM((n_tp * tokens, 2 * LANES), F32),
            pltpu.VMEM((slots, ff), F32),
            pltpu.VMEM((slots, ff), F32),
            pltpu.VMEM((slots, ff), BF16),
            pltpu.VMEM((width, ff), BF16),
            pltpu.VMEM((width, ff), BF16),
            pltpu.VMEM((ff, width), BF16),
            pltpu.VMEM((2 * LANES, width), BF16),
            pltpu.VMEM((width, 2 * LANES), BF16),
            pltpu.VMEM((LANES, width), BF16),
            pltpu.VMEM((tokens + HALO, width), BF16),
            pltpu.VMEM((4, n_z, 2, tokens, LANES), BF16),
            pltpu.VMEM((n_z, 2, 4, LANES, LANES), BF16),
            pltpu.VMEM((tokens, 4 * LANES), BF16),
            dma((16,)),
            dma((n_chunks, 3)),
            dma((n_chunks, 4)),
            dma((n_chunks, 4)),
            dma((n_chunks,)),
            dma((n_chunks,)),
            dma((n_chunks,)),
            dma((n_chunks,)),
            dma((n_chunks,)),
            dma((n_chunks, 3)),
            dma((n_chunks,)),
            dma((n_chunks, 4)),
            dma((n_chunks, 4)),
            dma((8,)),
            dma((8,)),
        ],
        compiler_params=pltpu.CompilerParams(
            collective_id=0, has_side_effects=True, vmem_limit_bytes=60 << 20
        ),
    )(
        moe_in, moe_gain.reshape(1, width), routes.T, route_score.T,
        mix_gain.reshape(1, width), pool_mat, pool_scale.reshape(1, -1),
        mix_in, mix_w_in, mix_w_out, exp_gate, exp_up, exp_down,
        shared_gate, shared_up, shared_down,
    )


def solution(mesh):
    n_ep, n_tp = mesh.shape["ep"], mesh.shape["tp"]
    return jax.shard_map(
        functools.partial(shards, n_ep, n_tp, 8),
        mesh=mesh,
        in_specs=(
            P(("ep", "tp"), None),
            P(),
            P("tp", None),
            P(),
            P(),
            P(None, "tp"),
            P(("ep", "tp"), None),
            P(),
            P("ep", None),
            P("ep", None),
            P(("ep", "tp"), None, None),
            P(("ep", "tp"), None, None),
            P(("ep", "tp"), None, None),
            P("tp", None),
            P("tp", None),
            P("tp", None),
        ),
        out_specs=(P(("ep", "tp"), None), P(("ep", "tp"), None)),
        check_vma=False,
    )
```

```python
import functools

import jax
import jax.numpy as jnp
from jax import lax
from jax.experimental import pallas as pl
from jax.experimental.pallas import tpu as pltpu
from jax.sharding import PartitionSpec as P

NORM_EPS = 1e-06
ROUTED_SCALE = 2.5
MESH = pl.DeviceIdType.MESH
F32 = jnp.float32
BF16 = jnp.bfloat16
HALO = 16
LANES = 128

LOOK = 1


def dot(a, b):
    return jnp.dot(a, b, preferred_element_type=F32)


def rms_rows(values, gain):
    floats = values.astype(F32)
    scaled = floats * lax.rsqrt(jnp.mean(floats * floats, axis=-1, keepdims=True) + NORM_EPS)
    return (scaled * gain).astype(BF16)


def kernel(
    n_ep, n_tp, n_chunks, cap,
    moe_in_hbm, moe_gain_hbm, routes_hbm, score_hbm, mix_gain_hbm, pool_mat_hbm, pool_scale_hbm,
    mix_in, mix_w_in, mix_w_out, exp_gate, exp_up, exp_down, sh_gate, sh_up, sh_down,
    mixed_ref, moe_ref,
    moe_in, moe_gain, routes, score, mix_gain, pool_mat, pool_scale, taken_ref,
    g_buf, out_buf, in_buf, res_buf, ret_buf, sib_buf, up_buf, dn_buf,
    p_mat, s_mat, spread, hid, hid_acc, gate_acc, up_acc, hidden,
    wg, wu, wd, sgu, sgt, sd, mx, wi, wo, pool_buf,
    local_sem, ag_send, ag_up, ag_dn, ag_sib, disp_send, disp_recv, ret_send, ret_recv,
    rs_send, rs_sib, rs_up, rs_dn, w_send, w_recv,
):
    tokens, width = moe_in.shape
    cols = width // n_chunks
    n_z = n_tp // 2
    half = tokens // 2
    slots = n_ep * cap
    ff = wd.shape[0]
    n_sh = sh_gate.shape[0]
    ep = lax.axis_index("ep")
    tp = lax.axis_index("tp")
    z = tp // 2
    k = tp % 2
    lin = ep * n_tp + tp

    def at_z(steps):
        return {"tp": ((z + steps + n_z) % n_z) * 2 + k}

    up, dn, sib = at_z(1), at_z(-1), {"tp": z * 2 + 1 - k}

    def ep_peer(offset):
        return {"ep": (ep + offset) % n_ep}

    after = lax.rem(lin + 1, n_ep * n_tp)
    before = lax.rem(lin + n_ep * n_tp - 1, n_ep * n_tp)

    def by_lin(index):
        return {"ep": index // n_tp, "tp": index % n_tp}

    def send(src, dst, send_sem, recv_sem, device):
        pltpu.make_async_remote_copy(
            src_ref=src, dst_ref=dst, send_sem=send_sem, recv_sem=recv_sem,
            device_id=device, device_id_type=MESH,
        ).start()

    def got(ref, sem):
        pltpu.make_async_remote_copy(
            src_ref=ref, dst_ref=ref, send_sem=sem, recv_sem=sem,
            device_id=sib, device_id_type=MESH,
        ).wait_recv()

    def sent(ref, sem):
        pltpu.make_async_remote_copy(
            src_ref=ref, dst_ref=ref, send_sem=sem, recv_sem=sem,
            device_id=sib, device_id_type=MESH,
        ).wait_send()

    barrier = pltpu.get_barrier_semaphore()

    def hello(device):
        pl.semaphore_signal(barrier, inc=1, device_id=device, device_id_type=MESH)

    for steps in range(1, n_z):
        hello(at_z(steps))
    hello(sib)
    hello(by_lin(after))
    hello(by_lin(before))

    @pl.loop(1, n_ep)
    def _(o):
        hello(ep_peer(o))

    q_rows = pl.ds(pl.multiple_of((ep % 4) * 32, 32), 32)
    q_grp = ep // 4
    e_rows = pl.ds(pl.multiple_of(ep * 32, 32), 32)
    early = [
        pltpu.make_async_copy(src, dst, local_sem.at[9 + j])
        for j, (src, dst) in enumerate((
            (moe_in_hbm, moe_in), (moe_gain_hbm, moe_gain), (routes_hbm, routes),
            (score_hbm, score), (mix_gain_hbm, mix_gain), (pool_mat_hbm, pool_mat),
            (pool_scale_hbm, pool_scale)))
    ]
    loads = [
        pltpu.make_async_copy(
            mix_w_in.at[q_rows, pl.ds(pl.multiple_of(q_grp * LANES, LANES), LANES)],
            wi.at[q_grp, z, k, q_rows, :], local_sem.at[0]),
        pltpu.make_async_copy(
            mix_w_out.at[e_rows, :], wo.at[z, k, q_grp, q_rows, :], local_sem.at[1]),
        pltpu.make_async_copy(sh_gate, sgu.at[pl.ds(0, n_sh), :], local_sem.at[2]),
        pltpu.make_async_copy(sh_up, sgu.at[pl.ds(LANES, n_sh), :], local_sem.at[3]),
        pltpu.make_async_copy(sh_down, sd.at[pl.ds(0, n_sh), :], local_sem.at[4]),
        pltpu.make_async_copy(exp_gate.at[0], wg, local_sem.at[5]),
        pltpu.make_async_copy(exp_up.at[0], wu, local_sem.at[6]),
        pltpu.make_async_copy(exp_down.at[0], wd, local_sem.at[7]),
        pltpu.make_async_copy(mix_in, mx.at[pl.ds(HALO, tokens), :], local_sem.at[8]),
    ]
    for load in early + loads:
        load.start()
    for load in early[:2]:
        load.wait()

    normed = rms_rows(moe_in[...], moe_gain[...])
    for f in range(n_chunks):
        g_buf[f, tp] = normed[:, f * cols:(f + 1) * cols]

    def own_pieces(f):
        own = g_buf.at[f, tp]
        for q in range(2):
            part = own.at[pl.ds(q * half, half), :]
            send(part, part, ag_send.at[f, 0], ag_up.at[f, 0, q], up)
            send(part, part, ag_send.at[f, 1], ag_dn.at[f, 0, q], dn)
        send(own, own, ag_send.at[f, 2], ag_sib.at[f], sib)

    wi_own = wi.at[q_grp, z, k, q_rows, :]
    wo_own = wo.at[z, k, q_grp, q_rows, :]
    x_at, y_at = ep % 4, ep // 4

    def weights_along_z():
        for steps in range(1, n_z):
            send(wi_own, wi_own, w_send.at[1], w_recv.at[1], at_z(steps))
            send(wo_own, wo_own, w_send.at[1], w_recv.at[1], at_z(steps))

    def along_x(steps):
        return {"ep": y_at * 4 + (x_at + steps) % 4}

    def along_y(steps):
        return {"ep": ((y_at + steps) % 4) * 4 + x_at}

    wi_set = wi.at[q_grp, :, k, q_rows, :]
    wo_set = wo.at[:, k, q_grp, q_rows, :]
    wi_row = wi.at[q_grp, :, k]
    wo_col = wo.at[:, k, :, q_rows, :]
    three = wo.at[:, 0, 0, pl.ds(0, 96), :]
    three_rows = wo.at[:, 0, pl.ds(0, 3)]

    def weights_first():
        got(wo.at[pl.ds(0, n_z - 1), 0, 0, pl.ds(0, 64), :], w_recv.at[1])
        for steps in range(1, 4):
            send(wi_set, wi_set, w_send.at[2], w_recv.at[2], along_x(steps))
            send(wo_set, wo_set, w_send.at[3], w_recv.at[3], along_y(steps))

    def weights_second():
        got(three, w_recv.at[2])
        got(three, w_recv.at[3])
        for steps in range(1, 4):
            send(wi_row, wi_row, w_send.at[6], w_recv.at[6], along_y(steps))
            send(wo_col, wo_col, w_send.at[7], w_recv.at[7], along_x(steps))

    def weights_sibling():
        got(three_rows, w_recv.at[6])
        got(three_rows, w_recv.at[7])
        send(wi.at[:, :, k], wi.at[:, :, k], w_send.at[4], w_recv.at[4], sib)
        send(wo.at[:, k], wo.at[:, k], w_send.at[5], w_recv.at[5], sib)

    def gather_step(i):
        @pl.when(i + LOOK < n_chunks)
        def _():
            own_pieces(i + LOOK)

        for hop in range(1, 4):
            f = i - hop

            @pl.when((f >= 0) & (f < n_chunks))
            def _():
                from_dn = g_buf.at[f, ((z - hop + n_z) % n_z) * 2 + k]
                from_up = g_buf.at[f, ((z + hop) % n_z) * 2 + k]
                for q in range(2):
                    part = from_dn.at[pl.ds(q * half, half), :]
                    got(part, ag_up.at[f, hop - 1, q])
                    if hop < 3 or q == 0:
                        send(part, part, ag_send.at[f, 0], ag_up.at[f, hop, q], up)
                    part = from_up.at[pl.ds(q * half, half), :]
                    got(part, ag_dn.at[f, hop - 1, q])
                    if hop < 3 or q == 1:
                        send(part, part, ag_send.at[f, 1], ag_dn.at[f, hop, q], dn)
                send(from_dn, from_dn, ag_send.at[f, 2], ag_sib.at[f], sib)
                send(from_up, from_up, ag_send.at[f, 2], ag_sib.at[f], sib)

        f4 = i - 4

        @pl.when((f4 >= 0) & (f4 < n_chunks))
        def _():
            far = g_buf.at[f4, ((z + 4) % n_z) * 2 + k]
            got(far.at[pl.ds(0, half), :], ag_up.at[f4, 3, 0])
            got(far.at[pl.ds(half, half), :], ag_dn.at[f4, 3, 1])
            send(far, far, ag_send.at[f4, 2], ag_sib.at[f4], sib)

    own_rows = pl.ds(pl.multiple_of(ep * cap, cap), cap)

    others = [(ep + step) % n_ep for step in range(1, n_ep)]

    def dispatch(f):
        got(g_buf.at[f, pl.ds(0, n_z)], ag_sib.at[f])
        rows_all = g_buf[f].reshape(n_tp * tokens, cols)
        out_buf[f] = dot(p_mat[...], rows_all).astype(BF16)

        for to in others:
            send(out_buf.at[f, pl.ds(pl.multiple_of(to * cap, cap), cap), :],
                 in_buf.at[f, own_rows, :], disp_send.at[f], disp_recv.at[f], {"ep": to})

        in_buf[f, own_rows, :] = out_buf[f, own_rows, :]

    def shared_up(first):
        base = 0 if first else n_chunks // 2

        @pl.loop(0, n_tp // 4)
        def _(m):
            x = jnp.concatenate(
                [g_buf[base + f, pl.ds(m * 4, 4)].reshape(4 * tokens, cols)
                 for f in range(n_chunks // 2)], axis=1)
            rows = pl.ds(pl.multiple_of(m * 4 * tokens, 4 * tokens), 4 * tokens)
            part = dot(x, sgt[base * cols:(base + n_chunks // 2) * cols, :])
            if first:
                hid_acc[rows, :] = part
            else:
                both = hid_acc[rows, :] + part
                units = (jax.nn.silu(both[:, :LANES]) * both[:, LANES:]).astype(BF16)
                for q in range(4):
                    spot = (q % 2) * n_z + m * 2 + q // 2
                    hid[pl.ds(pl.multiple_of(spot * tokens, tokens), tokens), :] = (
                        units[q * tokens:(q + 1) * tokens])

    def expert_up_part(f):
        got(in_buf.at[f, pl.ds(0, slots - cap), :], disp_recv.at[f])
        at = pl.ds(pl.multiple_of(f * cols, cols), cols)
        for w, acc in ((wg, gate_acc), (wu, up_acc)):
            part = dot(in_buf[f], w[at, :])

            @pl.when(f == 0)
            def _():
                acc[...] = part

            @pl.when(f > 0)
            def _():
                acc[...] += part

    def route_tables(b_from, b_to):
        wants = (lax.broadcasted_iota(jnp.int32, (tokens, slots), 1) % cap).astype(F32)
        rank_of = lax.broadcasted_iota(jnp.int32, (n_ep, cap, tokens), 1).astype(F32)
        ahead = (lax.broadcasted_iota(jnp.int32, (tokens, tokens), 0)
                 < lax.broadcasted_iota(jnp.int32, (tokens, tokens), 1)).astype(BF16)
        named = lax.broadcasted_iota(jnp.int32, (n_ep, tokens), 0) * n_tp + tp

        def block(b, taken):
            at = pl.ds(pl.multiple_of(b * tokens, tokens), tokens)
            pair = routes[:, at]
            marks = score[:, at].astype(F32)
            total = marks[0:1] + marks[1:2]
            first = pair[0:1] == named
            second = pair[1:2] == named
            mine = first | second
            flags = mine.astype(F32)
            place = dot(flags.astype(BF16), ahead) + taken
            code = jnp.where(mine, place, -1.0)
            weight = jnp.where(first, marks[0:1] / total * ROUTED_SCALE,
                               jnp.where(second, marks[1:2] / total * ROUTED_SCALE, 0.0))
            hot = (code[:, None, :] == rank_of).astype(BF16)
            p_mat[:, at] = hot.reshape(slots, tokens)
            both = jnp.concatenate(
                [code, weight, jnp.zeros((LANES - 2 * n_ep, tokens), F32)], axis=0)
            turned = both.T.astype(BF16)
            ranks = dot(turned, spread[0])
            scale = dot(turned, spread[1])
            spot = (b % 2) * n_z + b // 2
            s_mat[pl.ds(pl.multiple_of(spot * tokens, tokens), tokens), :] = jnp.where(
                ranks == wants, scale, 0.0).astype(BF16)
            return taken + jnp.sum(flags, axis=1, keepdims=True)

        taken = lax.fori_loop(b_from, b_to, block, taken_ref[:, :1])
        taken_ref[...] = jnp.broadcast_to(taken, taken_ref.shape)

    pl.semaphore_wait(barrier, n_z - 1 + 3 + n_ep - 1)
    for f in range(LOOK):
        own_pieces(f)
    gather_step(0)
    loads[0].wait()
    loads[1].wait()
    send(mix_in.at[pl.ds(tokens - HALO, HALO), :], mx.at[pl.ds(0, HALO), :],
         w_send.at[0], w_recv.at[0], by_lin(after))
    lane = lax.broadcasted_iota(jnp.int32, (LANES, slots), 1)
    row = lax.broadcasted_iota(jnp.int32, (LANES, slots), 0)
    spread[0] = (row == lane // cap).astype(BF16)
    spread[1] = (row - n_ep == lane // cap).astype(BF16)
    taken_ref[...] = jnp.zeros_like(taken_ref)
    sgu[n_sh:LANES, :] = jnp.zeros((LANES - n_sh, width), BF16)
    sgu[LANES + n_sh:, :] = jnp.zeros((LANES - n_sh, width), BF16)
    sd[n_sh:, :] = jnp.zeros((LANES - n_sh, width), BF16)
    for load in early[2:] + loads[2:]:
        load.wait()
    for f in range(n_chunks):
        sgt[f * cols:(f + 1) * cols, :] = sgu[:, f * cols:(f + 1) * cols].T

    @pl.loop(1, n_chunks + 7)
    def _(i):
        gather_step(i)
        pl.when(i == n_chunks + 2)(weights_along_z)
        pl.when(i == n_chunks + 5)(weights_first)

        @pl.when(i < 5)
        def _():
            route_tables((i - 1) * (n_tp // 4), i * (n_tp // 4))

        f5 = i - 5

        @pl.when((f5 >= 0) & (f5 < n_chunks))
        def _():
            dispatch(f5)

        @pl.when(i == n_chunks + 4)
        def _():
            shared_up(True)

        f6 = i - 7

        @pl.when(f6 >= 0)
        def _():
            expert_up_part(f6)

    @pl.loop(0, 4)
    def _(m):
        tile = slots // 4
        rows = pl.ds(pl.multiple_of(m * tile, tile), tile)
        hidden[rows, :] = (jax.nn.silu(gate_acc[rows, :]) * up_acc[rows, :]).astype(BF16)

    def expert_down(f):
        at = pl.ds(pl.multiple_of(f * cols, cols), cols)
        res_buf[f] = dot(hidden[...], wd[:, at]).astype(BF16)

        for to in others:
            send(res_buf.at[f, pl.ds(pl.multiple_of(to * cap, cap), cap), :],
                 ret_buf.at[f, own_rows, :], ret_send.at[f], ret_recv.at[f], {"ep": to})

        ret_buf[f, own_rows, :] = res_buf[f, own_rows, :]

    def combine(f):
        got(ret_buf.at[f, pl.ds(0, slots - cap), :], ret_recv.at[f])
        at = pl.ds(pl.multiple_of(f * cols, cols), cols)
        back = ret_buf[f]
        down = sd[:, at]

        def half_of(core):
            @pl.loop(0, 2)
            def _(j):
                m = core * 2 + j
                many = n_z // 2 * tokens
                rows = pl.ds(pl.multiple_of(m * many, many), many)
                part = dot(s_mat[rows, :], back) + dot(hid[rows, :], down)
                g_buf[f, pl.ds(m * (n_z // 2), n_z // 2)] = (
                    part.astype(BF16).reshape(n_z // 2, tokens, cols))

        half_of(1 - k)
        send(g_buf.at[f, pl.ds((1 - k) * n_z, n_z)], sib_buf.at[f],
             rs_send.at[f, 2], rs_sib.at[f], sib)
        half_of(k)

    def spot_of(steps):
        return (z + steps + n_z) % n_z

    def plus(f, place, rows, other):
        here = g_buf[f, k * n_z + place, rows, :].astype(F32) + other.astype(F32)
        g_buf[f, k * n_z + place, rows, :] = here.astype(BF16)

    every = pl.ds(0, tokens)
    low = pl.ds(0, half)
    high = pl.ds(half, half)

    def scatter_step(i):
        f2 = i - 2

        @pl.when((f2 >= 0) & (f2 < n_chunks))
        def _():
            got(sib_buf.at[f2], rs_sib.at[f2])
            far = spot_of(4)
            plus(f2, far, every, sib_buf[f2, far])
            send(g_buf.at[f2, k * n_z + far, low, :], up_buf.at[f2, 0, low, :],
                 rs_send.at[f2, 0], rs_up.at[f2, 0, 0], up)
            send(g_buf.at[f2, k * n_z + far, high, :], dn_buf.at[f2, 0, high, :],
                 rs_send.at[f2, 1], rs_dn.at[f2, 0, 1], dn)

        for hop in (1, 2, 3):
            f = i - 2 - hop

            @pl.when((f >= 0) & (f < n_chunks))
            def _():
                u, d = spot_of(4 - hop), spot_of(hop - 4)

                def onward(place, buf, sem, way, peer, q):
                    rows = (low, high)[q]
                    if hop > 1 or q == way:
                        got(buf.at[f, hop - 1, rows, :], sem.at[f, hop - 1, q])
                        plus(f, place, rows, buf[f, hop - 1, rows, :])
                    send(g_buf.at[f, k * n_z + place, rows, :], buf.at[f, hop, rows, :],
                         rs_send.at[f, way], sem.at[f, hop, q], peer)

                if hop == 1:
                    onward(u, up_buf, rs_up, 0, up, 1)
                    onward(d, dn_buf, rs_dn, 1, dn, 0)
                    onward(u, up_buf, rs_up, 0, up, 0)
                    onward(d, dn_buf, rs_dn, 1, dn, 1)
                else:
                    for q in range(2):
                        onward(u, up_buf, rs_up, 0, up, q)
                        onward(d, dn_buf, rs_dn, 1, dn, q)

        f = i - 6

        @pl.when((f >= 0) & (f < n_chunks))
        def _():
            for q, rows in enumerate((low, high)):
                got(up_buf.at[f, 3, rows, :], rs_up.at[f, 3, q])
                got(dn_buf.at[f, 3, rows, :], rs_dn.at[f, 3, q])
            at = pl.ds(pl.multiple_of(f * cols, cols), cols)
            moe_ref[:, at] = (g_buf[f, k * n_z + z].astype(F32) + up_buf[f, 3].astype(F32)
                              + dn_buf[f, 3].astype(F32)).astype(BF16)

        @pl.when((f2 >= 0) & (f2 < n_chunks))
        def _():
            @pl.loop(5, n_z + 4)
            def _(s):
                place = lax.rem(z + s, n_z)
                plus(f2, place, every, sib_buf[f2, place])

    def mixer_norm():
        got(wi.at[:, :, 1 - k], w_recv.at[4])
        got(wo.at[:, 1 - k], w_recv.at[5])
        got(mx.at[pl.ds(0, HALO), :], w_recv.at[0])
        mx[...] = rms_rows(mx[...], mix_gain[...])

    def mixer_group(g):
        position = lin * tokens + lax.broadcasted_iota(jnp.int32, (tokens, LANES), 0)
        inside = (lax.broadcasted_iota(jnp.int32, (tokens + HALO, LANES), 0) >= HALO) | (lin > 0)
        projected = dot(mx[...], wi[g].reshape(width, LANES)).astype(BF16).astype(F32)
        projected = jnp.where(inside, projected, 0.0)
        run = projected
        for step in range(g + 1):
            run = run + pltpu.roll(run, 2 ** step, 0)
        counts = jnp.minimum(position + 1, 2 ** (g + 1)).astype(F32)
        pooled = run[HALO:] / counts - projected[HALO:]
        grouped = dot(pooled.astype(BF16), pool_mat[g])
        pool_buf[:, g * LANES:(g + 1) * LANES] = (
            grouped * pool_scale[:, g * LANES:(g + 1) * LANES]).astype(BF16)

    def mixer_out(part):
        @pl.loop(part * (n_tp // 4), (part + 1) * (n_tp // 4))
        def _(t):
            at = pl.ds(pl.multiple_of(t * LANES, LANES), LANES)
            w = wo[t // 2, t % 2].reshape(4 * LANES, LANES)
            mixed_ref[:, at] = dot(pool_buf[...], w).astype(BF16)

    def settle(f):
        sent(res_buf.at[f, pl.ds(0, slots - cap), :], ret_send.at[f])
        sent(g_buf.at[f, pl.ds(0, n_z - 1), pl.ds(0, half), :], rs_send.at[f, 0])
        sent(g_buf.at[f, pl.ds(0, n_z - 1), pl.ds(0, half), :], rs_send.at[f, 1])
        sent(sib_buf.at[f], rs_send.at[f, 2])

    expert_down(0)
    for f in range(n_chunks):
        sent(g_buf.at[f, pl.ds(0, n_z - 1), pl.ds(0, half), :], ag_send.at[f, 0])
        sent(g_buf.at[f, pl.ds(0, n_z - 1), pl.ds(0, half), :], ag_send.at[f, 1])
        sent(g_buf.at[f, pl.ds(0, n_z)], ag_send.at[f, 2])
    expert_down(1)
    shared_up(False)

    @pl.loop(2, 5)
    def _(f):
        expert_down(f)

    @pl.loop(1, n_chunks + 6)
    def _(i):
        scatter_step(i)

        @pl.when(i <= n_chunks)
        def _():
            combine(i - 1)
            sent(out_buf.at[i - 1, pl.ds(0, slots - cap), :], disp_send.at[i - 1])

        @pl.when(i + 4 < n_chunks)
        def _():
            expert_down(i + 4)

        pl.when(i == 3)(weights_second)
        pl.when(i == n_chunks)(weights_sibling)

        @pl.when(i == n_chunks + 1)
        def _():
            mixer_norm()
            mixer_group(0)
            mixer_group(1)

        @pl.when(i == n_chunks + 2)
        def _():
            mixer_group(2)
            mixer_group(3)
            mixer_out(0)

        @pl.when(i == n_chunks + 3)
        def _():
            mixer_out(1)
            mixer_out(2)

        @pl.when(i == n_chunks + 4)
        def _():
            mixer_out(3)

        @pl.when(i > 6)
        def _():
            settle(i - 7)

        @pl.when(i == n_chunks + 4)
        def _():
            sent(mx.at[pl.ds(0, HALO), :], w_send.at[0])
            sent(wo.at[pl.ds(0, n_z - 1), 0, 0, pl.ds(0, 64), :], w_send.at[1])
            sent(three, w_send.at[2])
            sent(three, w_send.at[3])
            sent(three_rows, w_send.at[6])
            sent(three_rows, w_send.at[7])
            sent(wi.at[:, :, k], w_send.at[4])
            sent(wo.at[:, k], w_send.at[5])

    settle(n_chunks - 1)


def shards(
    n_ep, n_tp, n_chunks,
    mix_in, mix_gain, mix_w_in, pool_mat, pool_scale, mix_w_out, moe_in, moe_gain,
    routes, route_score, exp_gate, exp_up, exp_down, shared_gate, shared_up, shared_down,
):
    tokens, width = moe_in.shape
    cap = 2 * routes.shape[0] * routes.shape[1] // (n_ep * n_tp)
    slots = n_ep * cap
    ff = exp_gate.shape[2]
    cols = width // n_chunks
    n_z = n_tp // 2
    hbm = pl.BlockSpec(memory_space=pl.ANY)
    dma = pltpu.SemaphoreType.DMA
    big = (n_chunks, n_tp, tokens, cols)
    return pl.pallas_call(
        functools.partial(kernel, n_ep, n_tp, n_chunks, cap),
        out_shape=(
            pltpu.VMEM((tokens, width), BF16),
            pltpu.VMEM((tokens, width), BF16),
        ),
        in_specs=[hbm] * 16,
        out_specs=(pl.BlockSpec(memory_space=pltpu.VMEM),) * 2,
        scratch_shapes=[
            pltpu.VMEM((tokens, width), BF16),
            pltpu.VMEM((1, width), F32),
            pltpu.VMEM((2, routes.shape[0]), jnp.int32),
            pltpu.VMEM((2, routes.shape[0]), BF16),
            pltpu.VMEM((1, width), F32),
            pltpu.VMEM(pool_mat.shape, BF16),
            pltpu.VMEM((1, pool_scale.shape[0]), F32),
            pltpu.VMEM((n_ep, LANES), F32),
            pltpu.VMEM(big, BF16),
            pltpu.VMEM((n_chunks, slots, cols), BF16),
            pltpu.VMEM((n_chunks, slots, cols), BF16),
            pltpu.VMEM((n_chunks, slots, cols), BF16),
            pltpu.VMEM((n_chunks, slots, cols), BF16),
            pltpu.VMEM((n_chunks, n_z, tokens, cols), BF16),
            pltpu.VMEM((n_chunks, 4, tokens, cols), BF16),
            pltpu.VMEM((n_chunks, 4, tokens, cols), BF16),
            pltpu.VMEM((slots, n_tp * tokens), BF16),
            pltpu.VMEM((n_tp * tokens, slots), BF16),
            pltpu.VMEM((2, LANES, slots), BF16),
            pltpu.VMEM((n_tp * tokens, LANES), BF16),
            pltpu.VMEM((n_tp * tokens, 2 * LANES), F32),
            pltpu.VMEM((slots, ff), F32),
            pltpu.VMEM((slots, ff), F32),
            pltpu.VMEM((slots, ff), BF16),
            pltpu.VMEM((width, ff), BF16),
            pltpu.VMEM((width, ff), BF16),
            pltpu.VMEM((ff, width), BF16),
            pltpu.VMEM((2 * LANES, width), BF16),
            pltpu.VMEM((width, 2 * LANES), BF16),
            pltpu.VMEM((LANES, width), BF16),
            pltpu.VMEM((tokens + HALO, width), BF16),
            pltpu.VMEM((4, n_z, 2, tokens, LANES), BF16),
            pltpu.VMEM((n_z, 2, 4, LANES, LANES), BF16),
            pltpu.VMEM((tokens, 4 * LANES), BF16),
            dma((16,)),
            dma((n_chunks, 3)),
            dma((n_chunks, 4, 2)),
            dma((n_chunks, 4, 2)),
            dma((n_chunks,)),
            dma((n_chunks,)),
            dma((n_chunks,)),
            dma((n_chunks,)),
            dma((n_chunks,)),
            dma((n_chunks, 3)),
            dma((n_chunks,)),
            dma((n_chunks, 4, 2)),
            dma((n_chunks, 4, 2)),
            dma((8,)),
            dma((8,)),
        ],
        compiler_params=pltpu.CompilerParams(
            collective_id=0, has_side_effects=True, vmem_limit_bytes=60 << 20
        ),
    )(
        moe_in, moe_gain.reshape(1, width), routes.T, route_score.T,
        mix_gain.reshape(1, width), pool_mat, pool_scale.reshape(1, -1),
        mix_in, mix_w_in, mix_w_out, exp_gate, exp_up, exp_down,
        shared_gate, shared_up, shared_down,
    )


def solution(mesh):
    n_ep, n_tp = mesh.shape["ep"], mesh.shape["tp"]
    return jax.shard_map(
        functools.partial(shards, n_ep, n_tp, 8),
        mesh=mesh,
        in_specs=(
            P(("ep", "tp"), None),
            P(),
            P("tp", None),
            P(),
            P(),
            P(None, "tp"),
            P(("ep", "tp"), None),
            P(),
            P("ep", None),
            P("ep", None),
            P(("ep", "tp"), None, None),
            P(("ep", "tp"), None, None),
            P(("ep", "tp"), None, None),
            P("tp", None),
            P("tp", None),
            P("tp", None),
        ),
        out_specs=(P(("ep", "tp"), None), P(("ep", "tp"), None)),
        check_vma=False,
    )
```
